32 devices in a mesh: ep: 8 (over z, x), tp: 4 (over y, core).
Axes of the slice: x: 2, y: 2, z: 4, core: 2. Of those that a mesh axis runs over, the one named last changes fastest.
Arguments:
- x_attend: bfloat16 [4096, 2048], P('ep'), may hold values from -6 to 6
- attend_gain: float32 [2048], replicated, may hold values from 0.1 to 1.9
- w_query: bfloat16 [2048, 1024], P(None, 'tp'), may hold values from -0.125 to 0.125
- w_key: bfloat16 [2048, 512], P(None, 'tp'), may hold values from -0.125 to 0.125
- w_value: bfloat16 [2048, 512], P(None, 'tp'), may hold values from -0.125 to 0.125
- query_gain: float32 [64], replicated, may hold values from 0.1 to 1.9
- key_gain: float32 [64], replicated, may hold values from 0.1 to 1.9
- sink_logit: float32 [16], P('tp'), may hold values from 4 to 8
- w_output: bfloat16 [1024, 2048], P('tp'), may hold values from -1.5 to 1.5
- x_experts: bfloat16 [3072, 2048], P('ep'), may hold values from -6 to 6
- expert_gain: float32 [2048], replicated, may hold values from 0.1 to 1.9
- routes: int32 [3072, 2], P('ep'), may hold values from 0 to 7, all different within a row; in each aligned block of 384 rows (0 to 383, 384 to 767, ...) at most 144 rows name the same one
- group_prob: float32 [3072], P('ep'), may hold values from 0.3 to 1
- expert_prob: float32 [3072, 2], P('ep'), may hold values from 0.05 to 1
- w_gate: bfloat16 [8, 2048, 1024], P('ep', None, 'tp'), may hold values from -0.125 to 0.125
- w_up: bfloat16 [8, 2048, 1024], P('ep', None, 'tp'), may hold values from -0.125 to 0.125
- w_down: bfloat16 [8, 1024, 2048], P('ep', 'tp'), may hold values from -0.1875 to 0.1875
Outputs:
- attend_out: bfloat16 [4096, 2048], P(('ep', 'tp'))
- expert_out: bfloat16 [3072, 2048], P('ep', 'tp')
The draws below stay inside these ranges and needn't reach their ends.
Inputs may be any that keep to these rules, and one draw needn't show every extreme that they name: `routes`: each row names 2 different experts. Among the rows of one device no expert is named more than 144 times, and in every draw some expert is named exactly 144 times by one device's rows.
All inputs are finite; a program needn't handle non-finite values.
Results may differ from the reference program's by a relative error of at most 0.012.
Values may be sent and summed in bfloat16 or wider, within the bound.
A program may use at most 64 MiB of HBM per device.

```python
import math
import jax
import jax.numpy as jnp
import numpy as np
from jax import lax

D = 2048
HEADS = 16
KV_HEADS = 8
HEAD_DIM = 64
FF = 1024
TOPK = 2
WINDOW = 128
GRID_W = 64
TOK_A = 512
TOK_M = 384
EXPERTS = 8
CAP = 144
TOKENS_A = 4096
TOKENS_M = 3072
N_EP = 8
N_TP = 4


def levels(rng, shape, pieces, smallest, high):
    factor_of = 1.0
    for dim, blocks in pieces:
        heights = jax.random.uniform(jax.random.fold_in(jax.random.fold_in(rng, 6), dim), (blocks,), jnp.float32, smallest / len(pieces), high / len(pieces))
        factor_of = factor_of * jnp.repeat(jnp.exp(heights), shape[dim] // blocks).reshape((-1,) + (1,) * (len(shape) - 1 - dim))
    return factor_of


def assign_block(rng, own, number, rows, amount, top, reach, slope):
    ranking = jax.random.permutation(rng, amount)
    heavy_load, ordinary = shares(amount, rows * top, reach, slope, True), shares(amount, rows * top, reach, slope, False)
    places = jnp.arange(amount)

    def named(tallies, offset_by):
        used = int((tallies > 0).sum())
        fixed = max(1, used // 4)
        moved = fixed + (places - fixed + offset_by * (used - fixed)) % max(1, amount - fixed)
        return jnp.zeros((amount,), jnp.int32).at[ranking[jnp.where(places < fixed, places, moved)]].set(jnp.asarray(tallies, jnp.int32))

    tallies = jnp.where(number % 4 == 0, named(heavy_load, number // 4), named(ordinary, number - number // 4 - 1))
    mixed = jax.random.permutation(jax.random.fold_in(own, 3), amount)
    giver, sink = mixed[0:amount // 2 * 2:2], mixed[1:amount // 2 * 2:2]
    slack = jnp.minimum(tallies[giver] - 1, reach - tallies[sink]) // 2
    slack = jnp.where((giver == ranking[0]) | (sink == ranking[0]) | (tallies[sink] == 0), 0, jnp.maximum(slack, 0))
    moved = jax.random.randint(jax.random.fold_in(own, 4), (amount // 2,), 0, 1 << 20) % (slack + 1)
    tallies = tallies.at[giver].add(-moved).at[sink].add(moved)
    labels = jnp.searchsorted(jnp.cumsum(tallies), jnp.arange(rows * top), side="right").astype(jnp.int32)
    listing = labels.reshape(top, rows).T
    listing = listing[jax.random.permutation(jax.random.fold_in(own, 1), rows)]
    offset_by = jax.random.randint(jax.random.fold_in(own, 2), (rows, 1), 0, top)
    return jnp.take_along_axis(listing, (jnp.arange(top)[None, :] + offset_by) % top, axis=1)


def shares(amount, total, reach, skew, full):
    loads = [(1 << 20) // math.isqrt(grade ** skew) + 1 for grade in range(1, amount + 1)]
    largest = reach if full else min(reach, max(-(-total // amount), total * loads[0] // sum(loads)))
    least = 1 if total - largest >= amount - 1 else 0
    holding, surplus = [largest] + [least] * (amount - 1), total - largest - least * (amount - 1)
    while surplus > 0:
        free = [i for i in range(1, amount) if holding[i] < largest] or [i for i in range(1, amount) if holding[i] < reach]
        whole, remaining = sum([loads[i] for i in free]), surplus
        for i in free:
            extra = min(reach - holding[i], max(1, remaining * loads[i] // whole), surplus)
            holding[i] = holding[i] + extra
            surplus = surplus - extra
    return np.array(holding)


def gaussian(key, dims, width, bound, cuts=(), kind=jnp.bfloat16):
    level = levels(key, dims, cuts, -0.22, 0.18) if cuts else 1.0
    values = jax.random.normal(key, dims, jnp.float32) * width * level
    return jnp.minimum(jnp.maximum(values, -bound), bound).astype(kind)


def setup_inputs(seed: int = 0) -> dict:
    arg_keys = jax.random.split(jax.random.key(seed), 18)
    x_attend = gaussian(arg_keys[0], (TOKENS_A, D), 1.0, 6.0, ((0, 8),))
    attend_gain = jnp.clip(1.0 + 0.18 * jax.random.normal(arg_keys[1], (D,), jnp.float32), 0.1, 1.9)
    w_query = gaussian(arg_keys[2], (D, HEADS * HEAD_DIM), D ** -0.5, 0.125, ((1, 4),))
    w_key = gaussian(arg_keys[3], (D, KV_HEADS * HEAD_DIM), D ** -0.5, 0.125, ((1, 4),))
    w_value = gaussian(arg_keys[4], (D, KV_HEADS * HEAD_DIM), D ** -0.5, 0.125, ((1, 4),))
    query_gain = jnp.clip(1.0 + 0.18 * jax.random.normal(arg_keys[5], (HEAD_DIM,), jnp.float32), 0.1, 1.9)
    key_gain = jnp.clip(1.0 + 0.18 * jax.random.normal(arg_keys[6], (HEAD_DIM,), jnp.float32), 0.1, 1.9)
    sink_logit = jnp.clip(4.0 + 4.0 * jax.random.uniform(arg_keys[7], (HEADS,), jnp.float32) ** levels(arg_keys[7], (HEADS,), ((0, 4),), -0.2, 0.2), 4.0, 8.0)
    w_output = gaussian(arg_keys[8], (HEADS * HEAD_DIM, D), (HEAD_DIM // 4) ** -0.5, 1.5, ((0, 4),))
    x_experts = gaussian(arg_keys[9], (TOKENS_M, D), 1.0, 6.0, ((0, 8),))
    expert_gain = jnp.clip(1.0 + 0.18 * jax.random.normal(arg_keys[10], (D,), jnp.float32), 0.1, 1.9)
    routes_keys = jax.random.split(jax.random.fold_in(arg_keys[11], 1), TOKENS_M // TOK_M)
    routes_turns = jax.random.permutation(jax.random.fold_in(arg_keys[11], 3), TOKENS_M // TOK_M)
    routes = jax.vmap(lambda own, number: assign_block(jax.random.fold_in(arg_keys[11], 2), own, number, TOK_M, EXPERTS, TOPK, CAP, 2))(routes_keys, routes_turns).reshape((TOKENS_M, TOPK))
    group_prob = jnp.clip(0.3 + 0.7 * jax.random.uniform(arg_keys[12], (TOKENS_M,), jnp.float32) ** levels(arg_keys[12], (TOKENS_M,), ((0, 8),), -0.2, 0.2), 0.3, 1.0)
    expert_prob = jnp.clip(0.05 + 0.95 * jax.random.uniform(arg_keys[13], (TOKENS_M, TOPK), jnp.float32) ** levels(arg_keys[13], (TOKENS_M, TOPK), ((0, 8),), -0.2, 0.2), 0.05, 1.0)
    w_gate = gaussian(arg_keys[14], (EXPERTS, D, FF), D ** -0.5, 0.125, ((0, 8), (2, 4)))
    w_up = gaussian(arg_keys[15], (EXPERTS, D, FF), D ** -0.5, 0.125, ((0, 8), (2, 4)))
    w_down = gaussian(arg_keys[16], (EXPERTS, FF, D), FF ** -0.5, 0.1875, ((0, 8), (1, 4)))
    return dict(x_attend=x_attend, attend_gain=attend_gain, w_query=w_query, w_key=w_key, w_value=w_value, query_gain=query_gain, key_gain=key_gain, sink_logit=sink_logit, w_output=w_output, x_experts=x_experts, expert_gain=expert_gain, routes=routes, group_prob=group_prob, expert_prob=expert_prob, w_gate=w_gate, w_up=w_up, w_down=w_down)


epsilon = 1e-06
rope_base = 10000.0

def rms_scale(inputs, gain):
    values_f = inputs.astype(jnp.float32)
    scaled = values_f * lax.rsqrt(lax.optimization_barrier(jnp.mean(values_f * values_f, axis=-1, keepdims=True)) + epsilon)
    return (scaled * gain).astype(jnp.bfloat16)

def rope_tables(positions):
    grid_rows = (positions // GRID_W).astype(jnp.float32)
    grid_cols = (positions % GRID_W).astype(jnp.float32)
    half_dim = HEAD_DIM // 2
    inverse = rope_base ** (-jnp.arange(0, half_dim, 2, dtype=jnp.float32) / half_dim)
    angles = jnp.concatenate([grid_rows[:, None] * inverse, grid_cols[:, None] * inverse], axis=-1)
    return (jnp.cos(angles), jnp.sin(angles))

def head_norm_rope(projected, gain, cosine, sine_tab):
    scaled = projected * lax.rsqrt(lax.optimization_barrier(jnp.mean(projected * projected, axis=-1, keepdims=True)) + epsilon) * gain
    first_half, second_half = jnp.split(scaled, 2, axis=-1)
    cos_b = cosine[:, None, :]
    sin_b = sine_tab[:, None, :]
    turned = jnp.concatenate([first_half * cos_b - second_half * sin_b, second_half * cos_b + first_half * sin_b], axis=-1)
    return turned.astype(jnp.bfloat16)

def slot_plan(route_block):
    flat_ids = route_block.reshape(-1).astype(jnp.int32)
    onehot = (flat_ids[:, None] == jnp.arange(EXPERTS, dtype=jnp.int32)[None, :]).astype(jnp.int32)
    rank_in = jnp.cumsum(onehot, axis=0) - onehot
    slot_pos = lax.optimization_barrier(jnp.sum(rank_in * onehot, axis=1))
    dest_slot = (flat_ids * CAP + slot_pos).astype(jnp.int32)
    owner_tok = (jnp.arange(TOK_M * TOPK, dtype=jnp.int32) // TOPK).astype(jnp.int32)
    slot_tok = jnp.full((EXPERTS * CAP,), TOK_M, jnp.int32).at[dest_slot].set(owner_tok)
    return (dest_slot, slot_tok)

def reference(x_attend, attend_gain, w_query, w_key, w_value, query_gain, key_gain, sink_logit, w_output, x_experts, expert_gain, routes, group_prob, expert_prob, w_gate, w_up, w_down):
    normed = rms_scale(x_attend, attend_gain)
    positions = jnp.arange(TOKENS_A, dtype=jnp.int32)
    cosine, sine_tab = rope_tables(positions)
    queries = head_norm_rope(jnp.dot(normed, w_query, preferred_element_type=jnp.float32).reshape(TOKENS_A, HEADS, HEAD_DIM), query_gain, cosine, sine_tab)
    key_rows = head_norm_rope(jnp.dot(normed, w_key, preferred_element_type=jnp.float32).reshape(TOKENS_A, KV_HEADS, HEAD_DIM), key_gain, cosine, sine_tab)
    values = jnp.dot(normed, w_value, preferred_element_type=jnp.float32).astype(jnp.bfloat16).reshape(TOKENS_A, KV_HEADS, HEAD_DIM)
    key_pad = jnp.pad(key_rows, ((WINDOW, WINDOW), (0, 0), (0, 0)))
    value_pad = jnp.pad(values, ((WINDOW, WINDOW), (0, 0), (0, 0)))
    group = HEADS // KV_HEADS
    sink_col = sink_logit.reshape(KV_HEADS, group)[:, :, None]

    def one_block(blk_idx):
        row_zero = (blk_idx * TOK_A).astype(jnp.int32)
        query_blk = lax.dynamic_slice_in_dim(queries, row_zero, TOK_A, 0).reshape(TOK_A, KV_HEADS, group, HEAD_DIM).astype(jnp.float32)
        key_blk = lax.dynamic_slice_in_dim(key_pad, row_zero, TOK_A + 2 * WINDOW, 0).astype(jnp.float32)
        value_blk = lax.dynamic_slice_in_dim(value_pad, row_zero, TOK_A + 2 * WINDOW, 0).astype(jnp.float32)
        scores = jnp.einsum('qhgd,khd->hgqk', query_blk, key_blk) * HEAD_DIM ** (-0.5)
        query_pos = row_zero + jnp.arange(TOK_A, dtype=jnp.int32)
        key_pos = row_zero - WINDOW + jnp.arange(TOK_A + 2 * WINDOW, dtype=jnp.int32)
        in_window = (jnp.abs(query_pos[:, None] - key_pos[None, :]) <= WINDOW) & (key_pos[None, :] >= 0) & (key_pos[None, :] < TOKENS_A)
        scores = jnp.where(in_window[None, None], scores, -1e+30)
        peak = jnp.maximum(lax.optimization_barrier(jnp.max(scores, axis=-1)), sink_col)[..., None]
        weights = jnp.exp(scores - peak)
        denominator = lax.optimization_barrier(jnp.sum(weights, axis=-1, keepdims=True)) + jnp.exp(sink_col[..., None] - peak)
        probs = (weights / denominator).astype(jnp.bfloat16)
        attended_blk = jnp.einsum('hgqk,khd->qhgd', probs.astype(jnp.float32), value_blk)
        return attended_blk.astype(jnp.bfloat16).reshape(TOK_A, HEADS * HEAD_DIM)
    attended = lax.map(one_block, jnp.arange(N_EP, dtype=jnp.int32)).reshape(TOKENS_A, HEADS * HEAD_DIM)
    head_cols = HEADS * HEAD_DIM // N_TP
    total = jnp.zeros((TOKENS_A, D), jnp.float32)
    for part_idx in range(N_TP):
        partial_value = jnp.dot(attended[:, part_idx * head_cols:(part_idx + 1) * head_cols], w_output[part_idx * head_cols:(part_idx + 1) * head_cols], preferred_element_type=jnp.float32)
        partial_value = lax.optimization_barrier(partial_value.astype(jnp.bfloat16))
        total = total + partial_value.astype(jnp.float32)
    attend_out = total.astype(jnp.bfloat16)
    moe_normed = rms_scale(x_experts, expert_gain).reshape(N_EP, TOK_M, D)
    route_blocks = routes.reshape(N_EP, TOK_M, TOPK)
    dest_slot, slot_tok = jax.vmap(slot_plan)(route_blocks)
    padded_rows = jnp.concatenate([moe_normed, jnp.zeros((N_EP, 1, D), jnp.bfloat16)], axis=1)
    outgoing = jax.vmap(lambda rows_all, index_all: rows_all[index_all])(padded_rows, slot_tok)
    inbound = outgoing.reshape(N_EP, EXPERTS, CAP, D).transpose(1, 0, 2, 3)
    unit_cols = FF // N_TP

    def one_expert(operands):
        rows_in, gate_mat, up_mat, down_mat = operands
        flat_rows = rows_in.reshape(N_EP * CAP, D)
        gate_act = jnp.dot(flat_rows, gate_mat, preferred_element_type=jnp.float32)
        up_act = jnp.dot(flat_rows, up_mat, preferred_element_type=jnp.float32)
        hidden = (jax.nn.silu(gate_act) * up_act).astype(jnp.bfloat16)
        summed = jnp.zeros((N_EP * CAP, D), jnp.float32)
        for part_idx in range(N_TP):
            partial_value = jnp.dot(hidden[:, part_idx * unit_cols:(part_idx + 1) * unit_cols], down_mat[part_idx * unit_cols:(part_idx + 1) * unit_cols], preferred_element_type=jnp.float32)
            partial_value = lax.optimization_barrier(partial_value.astype(jnp.bfloat16))
            summed = summed + partial_value.astype(jnp.float32)
        return summed.astype(jnp.bfloat16).reshape(N_EP, CAP, D)
    results = lax.map(one_expert, (inbound, w_gate, w_up, w_down))
    back_rows = results.transpose(1, 0, 2, 3).reshape(N_EP, EXPERTS * CAP, D)
    picked = jax.vmap(lambda rows_all, index_all: rows_all[index_all])(back_rows, dest_slot).astype(jnp.float32)
    route_weight = group_prob[:, None] * expert_prob / lax.optimization_barrier(jnp.sum(expert_prob, axis=1, keepdims=True))
    expert_out = lax.optimization_barrier(jnp.sum(picked.reshape(TOKENS_M, TOPK, D) * route_weight[:, :, None], axis=1)).astype(jnp.bfloat16)
    return (attend_out, expert_out)
```

```python
import functools

import jax
import jax.numpy as jnp
from jax import lax
from jax.experimental import pallas as pl
from jax.experimental.pallas import tpu as pltpu
from jax.sharding import PartitionSpec as P

HEAD_DIM = 64
WINDOW = 128
GRID_W = 64
MESH = pl.DeviceIdType.MESH
EPSILON = 1e-06
LOG_BASE = 9.210340371976184
ATTN_CHUNKS = 4
bf16, f32, i32 = jnp.bfloat16, jnp.float32, jnp.int32


def flip(a, b, count):
    total, bit = 0, 1
    while bit < count:
        total = total + lax.rem(a // bit + b // bit, 2) * bit
        bit *= 2
    return total


def iota(shape, dim):
    return lax.broadcasted_iota(i32, shape, dim)


def dot(a, b):
    return jnp.dot(a, b, preferred_element_type=f32)


def dot_nt(a, b):
    return lax.dot_general(a, b, (((1,), (1,)), ((), ())), preferred_element_type=f32)


def one_zero(mask):
    return jnp.where(mask, 1.0, 0.0).astype(bf16)


def rms_inplace(ref, gain_ref, chunk):
    def body(i, carry):
        rows = pl.ds(pl.multiple_of(i * chunk, chunk), chunk)
        v = ref[rows, :].astype(f32)
        scale = lax.rsqrt(jnp.mean(v * v, axis=-1, keepdims=True) + EPSILON)
        ref[rows, :] = (v * scale * gain_ref[...]).astype(bf16)
        return carry

    lax.fori_loop(0, ref.shape[0] // chunk, body, 0)


def fused_kernel(
    n_ep,
    xa_hbm, a_gain, wq_hbm, wk_hbm, wv_hbm, q_gain, k_gain, sink, wo_hbm,
    xe_hbm, e_gain, routes_t, group_p, expert_p, wg_hbm, wu_hbm, wd_hbm,
    out_ref, attn_out_ref,
    xa, wqkv, wo, xe, wgu, wd,
    ctab, stab, q_s, kv, halo, kd, ve, att,
    attn_ref, attn_in, attn_y_out, attn_y_in,
    rank_s, rank_tn, share_tn, mix,
    send_own, send_other, rows_buf, part_out, part_keep, part_in,
    y_out, y_own, y_in, final, back, total,
    l_sem,
    d_send, d_recv, e_send, e_recv, p_send, p_recv, y_send, y_recv,
    r_send, r_recv, c_send, c_recv, s_send, s_recv, f_send, f_recv,
    a_send, a_recv, b_send, b_recv, h_send, h_recv,
):
    me = lax.axis_index("ep")
    lane = lax.axis_index("tp")
    core = lax.rem(lane, 2)
    side = lane // 2
    other_core, other_side = 1 - core, 1 - side
    partner = 2 * side + other_core
    across = 2 * other_side + core
    capacity, width = send_own.shape[1:]
    half = n_ep // 2
    tokens = xa.shape[0]
    moe_tokens = xe.shape[0]
    kv_local, ext_rows, pair = kd.shape
    q_cols = q_s.shape[1]
    hidden_cols = wd.shape[0]

    def local(i, src, dst):
        return pltpu.make_async_copy(src, dst, l_sem.at[i])

    kw = wk_hbm.shape[1]
    loads = [
        local(0, xe_hbm, xe),
        local(1, wg_hbm, wgu.at[:, 0:hidden_cols]),
        local(2, wu_hbm, wgu.at[:, hidden_cols : 2 * hidden_cols]),
        local(3, wd_hbm, wd),
        local(4, xa_hbm, xa),
        local(5, wq_hbm, wqkv.at[:, 0:q_cols]),
        local(6, wk_hbm, wqkv.at[:, q_cols : q_cols + kw]),
        local(7, wv_hbm, wqkv.at[:, q_cols + kw : q_cols + 2 * kw]),
        local(8, wo_hbm, wo),
    ]
    loads[0].start()

    barrier = pltpu.get_barrier_semaphore()

    def greet(k, carry):
        pl.semaphore_signal(
            barrier, inc=1, device_id={"ep": flip(me, k, n_ep), "tp": lane}, device_id_type=MESH
        )
        return carry

    lax.fori_loop(1, n_ep, greet, 0)
    for peer in (partner, across):
        pl.semaphore_signal(barrier, inc=1, device_id={"ep": me, "tp": peer}, device_id_type=MESH)

    def remote(src, dst, sends, recvs, k, ep, tp):
        return pltpu.make_async_remote_copy(
            src_ref=src,
            dst_ref=dst,
            send_sem=sends.at[k],
            recv_sem=recvs.at[k],
            device_id={"ep": ep, "tp": tp},
            device_id_type=MESH,
        )

    def dispatch(k):
        dest = flip(me, k, n_ep)
        return remote(send_own.at[k], rows_buf.at[lane, k], d_send, d_recv, k, dest, lane)

    def dispatch_other(k):
        dest = flip(me, k, n_ep)
        return remote(send_other.at[k], rows_buf.at[across, k], e_send, e_recv, k, dest, lane)

    def to_partner(k):
        block = rows_buf.at[lane, k]
        return remote(block, block, p_send, p_recv, k, me, partner)

    def to_across(k):
        block = rows_buf.at[lane, k]
        return remote(block, block, y_send, y_recv, k, me, across)

    def relay(k):
        block = rows_buf.at[across, k]
        return remote(block, block, r_send, r_recv, k, me, partner)

    def sum_core(k):
        return remote(part_out.at[k], part_in.at[k], c_send, c_recv, k, me, partner)

    def sum_side(k):
        return remote(y_out.at[k], y_in.at[k], s_send, s_recv, k, me, across)

    def give_back(k):
        return remote(final.at[k], back.at[k], f_send, f_recv, k, flip(me, k, n_ep), lane)

    def attn_core(s):
        return remote(
            attn_ref.at[2 * s + other_core], attn_in.at[s], a_send, a_recv, s, me, partner
        )

    chunk_rows = attn_y_out.shape[1]

    def attn_side(c):
        return remote(attn_y_out.at[c], attn_y_in.at[c], b_send, b_recv, c, me, across)

    def halo_up():
        return remote(
            kv.at[tokens - WINDOW : tokens], halo.at[0], h_send, h_recv, 0, me + 1, lane
        )

    def halo_down():
        return remote(kv.at[0:WINDOW], halo.at[1], h_send, h_recv, 1, me - 1, lane)

    def plan():
        names = iota((n_ep, moe_tokens), 0)
        named = None
        share = jnp.zeros((n_ep, moe_tokens), f32)
        top = routes_t.shape[0]
        prob_sum = expert_p[0:1, :]
        for j in range(1, top):
            prob_sum = prob_sum + expert_p[j : j + 1, :]
        for j in range(top):
            chosen = routes_t[j : j + 1, :] == names
            weight = group_p[...] * expert_p[j : j + 1, :] / prob_sum
            share = share + jnp.where(chosen, weight, 0.0)
            named = chosen if named is None else named | chosen
        before = one_zero(iota((moe_tokens, moe_tokens), 0) < iota((moe_tokens, moe_tokens), 1))
        same = one_zero(iota((moe_tokens, moe_tokens), 0) == iota((moe_tokens, moe_tokens), 1))
        rank = jnp.where(named, dot(one_zero(named), before), -1.0)
        rank_s[...] = rank
        rank_tn[...] = dot_nt(same, rank.astype(bf16))
        share_tn[...] = dot_nt(same, share.astype(bf16))

    def pick(k):
        row = rank_s[pl.ds(flip(me, k, n_ep), 1), :]
        return one_zero(row == iota((capacity, moe_tokens), 0).astype(f32))

    def gathered(chosen, quarter):
        start = pl.multiple_of(quarter * width, width)
        return dot(chosen, xe[:, pl.ds(start, width)]).astype(bf16)

    def D(k, near):
        chosen = pick(k)
        send_own[k] = gathered(chosen, lane)
        dispatch(k).start()
        if near:
            send_other[k] = gathered(chosen, across)
            dispatch_other(k).start()

    def L0():
        chosen = pick(0)
        rows_buf[lane, 0] = gathered(chosen, lane)
        to_partner(0).start()
        rows_buf[across, 0] = gathered(chosen, across)
        relay(0).start()

    def build_mix():
        columns = iota((moe_tokens, n_ep), 1)
        slots = iota((moe_tokens, capacity), 1).astype(f32)

        def body(e, carry):
            rank = jnp.sum(jnp.where(columns == e, rank_tn[...], 0.0), axis=1, keepdims=True)
            share = jnp.sum(jnp.where(columns == e, share_tn[...], 0.0), axis=1, keepdims=True)
            mix[e] = jnp.where(rank == slots, share, 0.0).astype(bf16)
            return carry

        lax.fori_loop(0, n_ep, body, 0)

    def A(k, near):
        dispatch(k).wait_recv()
        if near:
            to_partner(k).start()
            dispatch_other(k).wait_recv()
            relay(k).start()
        else:
            to_across(k).start()
            to_partner(k).start()

    def B(k):
        to_across(k).wait_recv()
        relay(k).start()

    def C(k):
        to_partner(k).wait_recv()
        relay(k).wait_recv()
        rows = jnp.concatenate([rows_buf[q, k] for q in range(4)], axis=1)
        acts = dot(rows, wgu[...])
        gate, up = acts[:, 0:hidden_cols], acts[:, hidden_cols:]
        hidden = (gate / (1.0 + jnp.exp(-gate)) * up).astype(bf16)
        for c, target in ((other_core, part_out), (core, part_keep)):
            for s in range(2):
                start = pl.multiple_of((2 * s + c) * width, width)
                target[k, s] = dot(hidden, wd[:, pl.ds(start, width)]).astype(bf16)
            if target is part_out:
                sum_core(k).start()

    def E(k):
        sum_core(k).wait_recv()
        y_out[k] = (
            part_keep[k, other_side].astype(f32) + part_in[k, other_side].astype(f32)
        ).astype(bf16)
        sum_side(k).start()
        y_own[k] = part_keep[k, side].astype(f32) + part_in[k, side].astype(f32)

    def F(k, own):
        sum_side(k).wait_recv()
        final[k] = (y_own[k] + y_in[k].astype(f32)).astype(bf16)
        if own:
            total[...] = dot(mix[me], final[0])
        else:
            give_back(k).start()

    def G(k):
        give_back(k).wait_recv()
        total[...] += dot(mix[flip(me, k, n_ep)], back[k])

    def rope_tables():
        lanes = lax.rem(iota((GRID_W, pair), 1), HEAD_DIM // 2)
        quarter = HEAD_DIM // 4
        inverse = jnp.exp(lax.rem(lanes, quarter).astype(f32) * (-LOG_BASE / quarter))
        by_row = lanes < quarter
        grid_rows = tokens // GRID_W
        first = me * grid_rows
        col_angle = iota((GRID_W, pair), 0).astype(f32) * inverse
        row_angle = (iota((grid_rows, pair), 0) + first).astype(f32) * inverse[0:grid_rows]
        for table, fn in ((ctab, jnp.cos), (stab, jnp.sin)):
            cols, rows = fn(col_angle), fn(row_angle)
            for r in range(grid_rows):
                table[r * GRID_W : (r + 1) * GRID_W, :] = jnp.where(
                    by_row, rows[r : r + 1, :], cols
                )

    def qkv():
        step = min(256, tokens)
        lanes = iota((1, pair), 1)
        low = lax.rem(lanes, HEAD_DIM) < HEAD_DIM // 2
        ones = one_zero(
            lax.rem(iota((2 * pair, pair), 0), pair) // HEAD_DIM
            == iota((2 * pair, pair), 1) // HEAD_DIM
        )
        gain_q = jnp.concatenate([q_gain[...]] * (pair // HEAD_DIM), axis=1)
        gain_k = jnp.concatenate([k_gain[...]] * (pair // HEAD_DIM), axis=1)

        def turned(x, gain, rows):
            square = x * x
            high = square.astype(bf16)
            rest = (square - high.astype(f32)).astype(bf16)
            mean = dot(jnp.concatenate([high, rest], axis=1), ones) * (1.0 / HEAD_DIM)
            scaled = x * lax.rsqrt(mean + EPSILON) * gain
            swapped = jnp.where(
                low,
                -pltpu.roll(scaled, pair - HEAD_DIM // 2, 1),
                pltpu.roll(scaled, HEAD_DIM // 2, 1),
            )
            return scaled * ctab[rows, :] + swapped * stab[rows, :]

        def body(i, carry):
            rows = pl.ds(pl.multiple_of(i * step, step), step)
            x = dot(xa[rows, :], wqkv[...])
            for g in range(q_cols // pair):
                span = slice(g * pair, (g + 1) * pair)
                q_s[rows, span] = (
                    turned(x[:, span], gain_q, rows) * HEAD_DIM ** (-0.5)
                ).astype(bf16)
            for g in range(kw // pair):
                span = slice(g * pair, (g + 1) * pair)
                k_span = slice(q_cols + g * pair, q_cols + (g + 1) * pair)
                kv[rows, span] = turned(x[:, k_span], gain_k, rows).astype(bf16)
            kv[rows, kw : 2 * kw] = x[:, q_cols + kw :].astype(bf16)
            return carry

        lax.fori_loop(0, tokens // step, body, 0)

    def expand(src, start, rows):
        block = jnp.concatenate([src[:, 0:kw], src[:, kw : 2 * kw]], axis=0)
        source = iota((kw, kv_local * pair), 0)
        column = iota((kw, kv_local * pair), 1)
        spread = one_zero(source == column // pair * HEAD_DIM + lax.rem(column, HEAD_DIM))
        doubled = dot(block, spread).astype(bf16)
        for h in range(kv_local):
            span = slice(h * pair, (h + 1) * pair)
            kd[h, start : start + rows, :] = doubled[0:rows, span]
            ve[h, start : start + rows, 0:pair] = doubled[rows:, span]
            ve[h, start : start + rows, pair : 2 * pair] = jnp.ones((rows, pair), bf16)

    def blank(start):
        for h in range(kv_local):
            kd[h, start : start + WINDOW, :] = jnp.zeros((WINDOW, pair), bf16)
            ve[h, start : start + WINDOW, :] = jnp.zeros((WINDOW, 2 * pair), bf16)

    def halo_start():
        @pl.when(me < n_ep - 1)
        def _():
            halo_up().start()

        @pl.when(me > 0)
        def _():
            halo_down().start()

    def halo_finish():
        @pl.when(me > 0)
        def _():
            halo_up().wait_recv()
            expand(halo.at[0], 0, WINDOW)

        @pl.when(me == 0)
        def _():
            blank(0)

        @pl.when(me < n_ep - 1)
        def _():
            halo_down().wait_recv()
            expand(halo.at[1], WINDOW + tokens, WINDOW)

        @pl.when(me == n_ep - 1)
        def _():
            blank(WINDOW + tokens)

    def attend(first, count, stride):
        span = 3 * WINDOW
        lanes = iota((1, pair), 1)
        left = one_zero(lanes < HEAD_DIM)
        right = one_zero(lanes >= HEAD_DIM)
        query = lax.rem(iota((2 * WINDOW, span), 0), WINDOW)
        key = iota((2 * WINDOW, span), 1)
        seen = (key >= query) & (key <= query + 2 * WINDOW)

        def body(j, carry):
            start = pl.multiple_of((first + stride * j) * WINDOW, WINDOW)
            rows = pl.ds(start, WINDOW)
            keys = pl.ds(start, span)
            for h in range(kv_local):
                cols = slice(h * pair, (h + 1) * pair)
                heads = q_s[rows, cols]
                stacked = jnp.concatenate([heads * left, heads * right], axis=0)
                scores = dot_nt(stacked, kd[h, keys, :])
                weights = jnp.where(seen, jnp.exp(scores), 0.0).astype(bf16)
                mixed = dot(weights, ve[h, keys, :])
                sink_0 = jnp.exp(jnp.full((1, pair), sink[2 * h], f32))
                sink_1 = jnp.exp(jnp.full((1, pair), sink[2 * h + 1], f32))
                upper = mixed[0:WINDOW, 0:pair] / (mixed[0:WINDOW, pair:] + sink_0)
                lower = mixed[WINDOW:, 0:pair] / (mixed[WINDOW:, pair:] + sink_1)
                att[rows, cols] = jnp.where(lanes < HEAD_DIM, upper, lower).astype(bf16)
            return carry

        lax.fori_loop(0, count, body, 0)

    def project():
        tile = 2 * pair
        quarter = attn_ref.shape[1]

        def body(n, carry):
            cols = pl.ds(pl.multiple_of(n * tile, tile), tile)
            x = dot(att[...], wo[:, cols]).astype(bf16)
            for s in range(attn_ref.shape[0]):
                attn_ref[s, :, cols] = x[s * quarter : (s + 1) * quarter]
            return carry

        lax.fori_loop(0, wo.shape[1] // tile, body, 0)
        attn_core(0).start()
        attn_core(1).start()

    def attn_sum():
        attn_core(0).wait_recv()
        attn_core(1).wait_recv()

    def attn_cross(c):
        rows = slice(c * chunk_rows, (c + 1) * chunk_rows)
        attn_y_out[c] = (
            attn_ref[2 * other_side + core, rows].astype(f32)
            + attn_in[other_side, rows].astype(f32)
        ).astype(bf16)
        attn_side(c).start()

    def attn_final(c):
        rows = slice(c * chunk_rows, (c + 1) * chunk_rows)
        attn_side(c).wait_recv()
        attn_out_ref[rows] = (
            attn_ref[2 * side + core, rows].astype(f32)
            + attn_in[side, rows].astype(f32)
            + attn_y_in[c].astype(f32)
        ).astype(bf16)

    nb = tokens // WINDOW

    plan()
    loads[0].wait()
    for copy in loads[1:]:
        copy.start()
    rms_inplace(xe, e_gain, 32)
    pl.semaphore_wait(barrier, n_ep + 1)

    def load_ffn():
        for copy in loads[1:4]:
            copy.wait()

    def attention_front():
        for copy in loads[4:9]:
            copy.wait()
        rms_inplace(xa, a_gain, 32)
        rope_tables()
        qkv()

    if n_ep == 8:
        D(4, False)
        D(1, True)
        D(5, False)
        D(2, True)
        L0()
        load_ffn()
        C(0)
        attention_front()
        E(0)
        halo_start()
        D(6, False)
        D(3, True)
        D(7, False)
        expand(kv, WINDOW, tokens)
        attend(1, nb - 2, 1)
        A(1, True)
        A(4, False)
        C(1)
        build_mix()
        E(1)
        B(4)
        C(4)
        halo_finish()
        attend(0, 2, nb - 1)
        E(4)
        project()
        F(0, True)
        A(2, True)
        F(1, False)
        C(2)
        A(5, False)
        F(4, False)
        E(2)
        attn_sum()
        attn_cross(0)
        B(5)
        C(5)
        A(3, True)
        E(5)
        F(2, False)
        C(3)
        A(6, False)
        E(3)
        F(5, False)
        attn_cross(1)
        B(6)
        C(6)
        F(3, False)
        E(6)
        attn_cross(2)
        G(1)
        A(7, False)
        F(6, False)
        B(7)
        C(7)
        E(7)
        attn_cross(3)
        G(4)
        G(2)
        F(7, False)
        G(5)
        G(3)
        for c in range(ATTN_CHUNKS):
            attn_final(c)
        G(6)
        G(7)
    else:
        def each(low, high, fn):
            def body(k, carry):
                fn(k)
                return carry

            lax.fori_loop(low, high, body, 0)

        each(half, n_ep, lambda k: D(k, False))
        each(1, half, lambda k: D(k, True))
        L0()
        load_ffn()
        attention_front()
        halo_start()
        expand(kv, WINDOW, tokens)
        attend(1, nb - 2, 1)
        each(1, half, lambda k: A(k, True))
        each(half, n_ep, lambda k: A(k, False))
        halo_finish()
        attend(0, 2, nb - 1)
        project()
        build_mix()
        each(half, n_ep, B)
        each(0, n_ep, C)
        each(0, n_ep, E)
        attn_sum()
        F(0, True)
        each(1, n_ep, lambda k: F(k, False))
        for c in range(ATTN_CHUNKS):
            attn_cross(c)
        each(1, n_ep, G)
        for c in range(ATTN_CHUNKS):
            attn_final(c)

    out_ref[...] = total[...].astype(bf16)

    def drain(k, carry):
        @pl.when(k > 0)
        def _():
            dispatch(k).wait_send()
            give_back(k).wait_send()

        to_partner(k).wait_send()

        @pl.when(k >= half)
        def _():
            to_across(k).wait_send()

        @pl.when((k > 0) & (k < half))
        def _():
            dispatch_other(k).wait_send()

        relay(k).wait_send()
        sum_core(k).wait_send()
        sum_side(k).wait_send()
        return carry

    lax.fori_loop(0, n_ep, drain, 0)
    attn_core(0).wait_send()
    attn_core(1).wait_send()
    for c in range(ATTN_CHUNKS):
        attn_side(c).wait_send()

    @pl.when(me < n_ep - 1)
    def _():
        halo_up().wait_send()

    @pl.when(me > 0)
    def _():
        halo_down().wait_send()


def per_device(
    x_attend, attend_gain, w_query, w_key, w_value, query_gain, key_gain, sink_logit, w_output,
    x_experts, expert_gain, routes, group_prob, expert_prob, w_gate, w_up, w_down,
):
    tokens, model_width = x_attend.shape
    q_cols, kv_cols = w_query.shape[1], w_key.shape[1]
    kv_local = kv_cols // HEAD_DIM
    tp_count, n_ep = lax.axis_size("tp"), lax.axis_size("ep")
    moe_rows, top_count = routes.shape
    capacity = max(2, (3 * moe_rows * top_count + 2 * n_ep - 1) // (2 * n_ep))
    col_width = model_width // tp_count
    hidden_cols = w_gate.shape[2]
    slice_rows = tokens // tp_count
    ext = tokens + 2 * WINDOW
    pair = 2 * HEAD_DIM
    chunk = slice_rows // ATTN_CHUNKS
    vmem = pl.BlockSpec(memory_space=pltpu.VMEM)
    smem = pl.BlockSpec(memory_space=pltpu.SMEM)
    hbm = pl.BlockSpec(memory_space=pl.ANY)
    dma = pltpu.SemaphoreType.DMA

    def buf(*shape, dtype=bf16):
        return pltpu.VMEM(shape, dtype)

    expert_out, attend_out = pl.pallas_call(
        functools.partial(fused_kernel, n_ep),
        out_shape=(
            jax.ShapeDtypeStruct((moe_rows, col_width), bf16),
            jax.ShapeDtypeStruct((slice_rows, model_width), bf16),
        ),
        in_specs=[
            hbm, vmem, hbm, hbm, hbm, vmem, vmem, smem, hbm,
            hbm, vmem, vmem, vmem, vmem, hbm, hbm, hbm,
        ],
        out_specs=(vmem, vmem),
        scratch_shapes=[
            buf(tokens, model_width),
            buf(model_width, q_cols + 2 * kv_cols),
            buf(q_cols, model_width),
            buf(moe_rows, model_width),
            buf(model_width, 2 * hidden_cols),
            buf(hidden_cols, model_width),
            buf(tokens, pair, dtype=f32),
            buf(tokens, pair, dtype=f32),
            buf(tokens, q_cols),
            buf(tokens, 2 * kv_cols),
            buf(2, WINDOW, 2 * kv_cols),
            buf(kv_local, ext, pair),
            buf(kv_local, ext, 2 * pair),
            buf(tokens, q_cols),
            buf(tp_count, slice_rows, model_width),
            buf(2, slice_rows, model_width),
            buf(ATTN_CHUNKS, chunk, model_width),
            buf(ATTN_CHUNKS, chunk, model_width),
            buf(n_ep, moe_rows, dtype=f32),
            buf(moe_rows, n_ep, dtype=f32),
            buf(moe_rows, n_ep, dtype=f32),
            buf(n_ep, moe_rows, capacity),
            buf(n_ep, capacity, col_width),
            buf(n_ep // 2, capacity, col_width),
            buf(tp_count, n_ep, capacity, col_width),
            buf(n_ep, 2, capacity, col_width),
            buf(n_ep, 2, capacity, col_width),
            buf(n_ep, 2, capacity, col_width),
            buf(n_ep, capacity, col_width),
            buf(n_ep, capacity, col_width, dtype=f32),
            buf(n_ep, capacity, col_width),
            buf(n_ep, capacity, col_width),
            buf(n_ep, capacity, col_width),
            buf(moe_rows, col_width, dtype=f32),
            dma((9,)),
        ]
        + [dma((n_ep,))] * 16
        + [dma((2,))] * 2
        + [dma((ATTN_CHUNKS,))] * 2
        + [dma((2,))] * 2,
        compiler_params=pltpu.CompilerParams(
            collective_id=0, has_side_effects=True, vmem_limit_bytes=60 * 1024 * 1024
        ),
    )(
        x_attend, attend_gain[None], w_query, w_key, w_value, query_gain[None], key_gain[None],
        sink_logit, w_output, x_experts, expert_gain[None], routes.T, group_prob[None],
        expert_prob.T, w_gate[0], w_up[0], w_down[0],
    )
    return (attend_out, expert_out)


def solution(mesh):
    placed = (
        P("ep", None),
        P(),
        P(None, "tp"),
        P(None, "tp"),
        P(None, "tp"),
        P(),
        P(),
        P("tp"),
        P("tp", None),
        P("ep", None),
        P(),
        P("ep", None),
        P("ep"),
        P("ep", None),
        P("ep", None, "tp"),
        P("ep", None, "tp"),
        P("ep", "tp", None),
    )
    return jax.shard_map(
        per_device,
        mesh=mesh,
        in_specs=placed,
        out_specs=(P(("ep", "tp"), None), P("ep", "tp")),
        check_vma=False,
    )
```

```python
import functools

import jax
import jax.numpy as jnp
from jax import lax
from jax.experimental import pallas as pl
from jax.experimental.pallas import tpu as pltpu
from jax.sharding import PartitionSpec as P

HEAD_DIM = 64
WINDOW = 128
GRID_W = 64
MESH = pl.DeviceIdType.MESH
EPSILON = 1e-06
LOG_BASE = 9.210340371976184
ATTN_CHUNKS = 8
XE_PIECES = 3
bf16, f32, i32 = jnp.bfloat16, jnp.float32, jnp.int32


def flip(a, b, count):
    total, bit = 0, 1
    while bit < count:
        total = total + lax.rem(a // bit + b // bit, 2) * bit
        bit *= 2
    return total


def iota(shape, dim):
    return lax.broadcasted_iota(i32, shape, dim)


def dot(a, b):
    return jnp.dot(a, b, preferred_element_type=f32)


def dot_nt(a, b):
    return lax.dot_general(a, b, (((1,), (1,)), ((), ())), preferred_element_type=f32)


def one_zero(mask):
    return jnp.where(mask, 1.0, 0.0).astype(bf16)


def rms_inplace(ref, first, count, gain_ref):
    chunk = 32

    def body(i, carry):
        rows = pl.ds(pl.multiple_of(first + i * chunk, chunk), chunk)
        v = ref[rows, :].astype(f32)
        scale = lax.rsqrt(jnp.mean(v * v, axis=-1, keepdims=True) + EPSILON)
        ref[rows, :] = (v * scale * gain_ref[...]).astype(bf16)
        return carry

    lax.fori_loop(0, count // chunk, body, 0)


def fused_kernel(
    n_ep,
    xa_hbm, a_gain, wq_hbm, wk_hbm, wv_hbm, q_gain, k_gain, sink, wo_hbm,
    xe_hbm, e_gain, routes_t, group_hbm, expert_p, wg_hbm, wu_hbm, wd_hbm,
    out_ref, attn_out_ref,
    xa, wqkv, wo, xe, wgu, wd,
    ctab, stab, q_s, kv, halo, kd, ve, att,
    attn_ref, attn_in, attn_y_out, attn_y_in,
    group_p, rank_s, rank_tn, share_tn, mix,
    send_own, send_other, rows_buf, part_out, part_keep, part_in,
    y_out, y_own, y_in, final, back, total,
    l_sem, x_sem,
    d_send, d_recv, e_send, e_recv, p_send, p_recv, y_send, y_recv,
    r_send, r_recv, c_send, c_recv, s_send, s_recv, f_send, f_recv,
    a_send, a_recv, b_send, b_recv, h_send, h_recv,
):
    me = lax.axis_index("ep")
    lane = lax.axis_index("tp")
    core = lax.rem(lane, 2)
    side = lane // 2
    other_core, other_side = 1 - core, 1 - side
    partner = 2 * side + other_core
    across = 2 * other_side + core
    capacity, width = send_own.shape[1:]
    half = n_ep // 2
    tokens = xa.shape[0]
    moe_tokens = xe.shape[0]
    kv_local, ext_rows, pair = kd.shape
    q_cols = q_s.shape[1]
    hidden_cols = wd.shape[0]

    def local(i, src, dst):
        return pltpu.make_async_copy(src, dst, l_sem.at[i])

    kw = wk_hbm.shape[1]
    loads = [
        local(0, wg_hbm, wgu.at[:, 0:hidden_cols]),
        local(1, wu_hbm, wgu.at[:, hidden_cols : 2 * hidden_cols]),
        local(2, wd_hbm, wd),
        local(3, xa_hbm, xa),
        local(4, wq_hbm, wqkv.at[:, 0:q_cols]),
        local(5, wk_hbm, wqkv.at[:, q_cols : q_cols + kw]),
        local(6, wv_hbm, wqkv.at[:, q_cols + kw : q_cols + 2 * kw]),
        local(7, wo_hbm, wo),
        local(8, group_hbm, group_p.at[0]),
    ]
    loads[8].start()
    first_rows = moe_tokens // XE_PIECES
    pieces = [
        pltpu.make_async_copy(
            xe_hbm.at[i * first_rows : (i + 1) * first_rows],
            xe.at[i * first_rows : (i + 1) * first_rows],
            x_sem.at[i],
        )
        for i in range(XE_PIECES)
    ]
    for copy in pieces:
        copy.start()

    barrier = pltpu.get_barrier_semaphore()

    def greet(k, carry):
        pl.semaphore_signal(
            barrier, inc=1, device_id={"ep": flip(me, k, n_ep), "tp": lane}, device_id_type=MESH
        )
        return carry

    lax.fori_loop(1, n_ep, greet, 0)
    for peer in (partner, across):
        pl.semaphore_signal(barrier, inc=1, device_id={"ep": me, "tp": peer}, device_id_type=MESH)

    def remote(src, dst, sends, recvs, k, ep, tp):
        return pltpu.make_async_remote_copy(
            src_ref=src,
            dst_ref=dst,
            send_sem=sends.at[k],
            recv_sem=recvs.at[k],
            device_id={"ep": ep, "tp": tp},
            device_id_type=MESH,
        )

    def dispatch(k):
        dest = flip(me, k, n_ep)
        return remote(send_own.at[k], rows_buf.at[lane, k], d_send, d_recv, k, dest, lane)

    def dispatch_other(k):
        dest = flip(me, k, n_ep)
        return remote(send_other.at[k], rows_buf.at[across, k], e_send, e_recv, k, dest, lane)

    def to_partner(k):
        block = rows_buf.at[lane, k]
        return remote(block, block, p_send, p_recv, k, me, partner)

    def to_across(k):
        block = rows_buf.at[lane, k]
        return remote(block, block, y_send, y_recv, k, me, across)

    def relay(k):
        block = rows_buf.at[across, k]
        return remote(block, block, r_send, r_recv, k, me, partner)

    def sum_core(k):
        return remote(part_out.at[k], part_in.at[k], c_send, c_recv, k, me, partner)

    def sum_side(k):
        return remote(y_out.at[k], y_in.at[k], s_send, s_recv, k, me, across)

    def give_back(k):
        return remote(final.at[k], back.at[k], f_send, f_recv, k, flip(me, k, n_ep), lane)

    def attn_core(s):
        return remote(
            attn_ref.at[2 * s + other_core], attn_in.at[s], a_send, a_recv, s, me, partner
        )

    chunk_rows = attn_y_out.shape[1]

    def attn_side(c):
        return remote(attn_y_out.at[c], attn_y_in.at[c], b_send, b_recv, c, me, across)

    def halo_up():
        return remote(
            kv.at[tokens - WINDOW : tokens], halo.at[0], h_send, h_recv, 0, me + 1, lane
        )

    def halo_down():
        return remote(kv.at[0:WINDOW], halo.at[1], h_send, h_recv, 1, me - 1, lane)

    def plan():
        names = iota((n_ep, moe_tokens), 0)
        named = None
        share = jnp.zeros((n_ep, moe_tokens), f32)
        top = routes_t.shape[0]
        prob_sum = expert_p[0:1, :]
        for j in range(1, top):
            prob_sum = prob_sum + expert_p[j : j + 1, :]
        for j in range(top):
            chosen = routes_t[j : j + 1, :] == names
            weight = group_p[...] * expert_p[j : j + 1, :] / prob_sum
            share = share + jnp.where(chosen, weight, 0.0)
            named = chosen if named is None else named | chosen
        before = one_zero(iota((moe_tokens, moe_tokens), 0) < iota((moe_tokens, moe_tokens), 1))
        same = one_zero(iota((moe_tokens, moe_tokens), 0) == iota((moe_tokens, moe_tokens), 1))
        rank = jnp.where(named, dot(one_zero(named), before), -1.0)
        rank_s[...] = rank
        rank_tn[...] = dot_nt(same, rank.astype(bf16))
        share_tn[...] = dot_nt(same, share.astype(bf16))

    def pick(k):
        row = rank_s[pl.ds(flip(me, k, n_ep), 1), :]
        return one_zero(row == iota((capacity, moe_tokens), 0).astype(f32))

    def gathered(chosen, quarter):
        start = pl.multiple_of(quarter * width, width)
        return dot(chosen, xe[:, pl.ds(start, width)]).astype(bf16)

    def D(k, near):
        chosen = pick(k)
        send_own[k] = gathered(chosen, lane)
        dispatch(k).start()
        if near:
            send_other[k] = gathered(chosen, across)
            dispatch_other(k).start()

    def L0():
        chosen = pick(0)
        rows_buf[lane, 0] = gathered(chosen, lane)
        to_partner(0).start()
        rows_buf[across, 0] = gathered(chosen, across)
        relay(0).start()

    def build_mix():
        columns = iota((moe_tokens, n_ep), 1)
        slots = iota((moe_tokens, capacity), 1).astype(f32)

        def body(e, carry):
            rank = jnp.sum(jnp.where(columns == e, rank_tn[...], 0.0), axis=1, keepdims=True)
            share = jnp.sum(jnp.where(columns == e, share_tn[...], 0.0), axis=1, keepdims=True)
            mix[e] = jnp.where(rank == slots, share, 0.0).astype(bf16)
            return carry

        lax.fori_loop(0, n_ep, body, 0)

    def A(k, near):
        dispatch(k).wait_recv()
        if not near:
            to_across(k).start()
        to_partner(k).start()

    def Z(k):
        dispatch_other(k).wait_recv()
        relay(k).start()

    def B(k):
        to_across(k).wait_recv()
        relay(k).start()

    def C(k):
        to_partner(k).wait_recv()
        relay(k).wait_recv()
        rows = jnp.concatenate([rows_buf[q, k] for q in range(4)], axis=1)
        acts = dot(rows, wgu[...])
        gate, up = acts[:, 0:hidden_cols], acts[:, hidden_cols:]
        hidden = (gate / (1.0 + jnp.exp(-gate)) * up).astype(bf16)
        for c, target in ((other_core, part_out), (core, part_keep)):
            for s in range(2):
                start = pl.multiple_of((2 * s + c) * width, width)
                target[k, s] = dot(hidden, wd[:, pl.ds(start, width)]).astype(bf16)
            if target is part_out:
                sum_core(k).start()

    def E(k):
        sum_core(k).wait_recv()
        y_out[k] = (
            part_keep[k, other_side].astype(f32) + part_in[k, other_side].astype(f32)
        ).astype(bf16)
        sum_side(k).start()
        y_own[k] = part_keep[k, side].astype(f32) + part_in[k, side].astype(f32)

    def F(k, own):
        sum_side(k).wait_recv()
        final[k] = (y_own[k] + y_in[k].astype(f32)).astype(bf16)
        if own:
            total[...] = dot(mix[me], final[0])
        else:
            give_back(k).start()

    def G(k):
        give_back(k).wait_recv()
        total[...] += dot(mix[flip(me, k, n_ep)], back[k])

    def rope_tables():
        lanes = lax.rem(iota((GRID_W, pair), 1), HEAD_DIM // 2)
        quarter = HEAD_DIM // 4
        inverse = jnp.exp(lax.rem(lanes, quarter).astype(f32) * (-LOG_BASE / quarter))
        by_row = lanes < quarter
        grid_rows = tokens // GRID_W
        first = me * grid_rows
        col_angle = iota((GRID_W, pair), 0).astype(f32) * inverse
        row_angle = (iota((grid_rows, pair), 0) + first).astype(f32) * inverse[0:grid_rows]
        for table, fn in ((ctab, jnp.cos), (stab, jnp.sin)):
            cols, rows = fn(col_angle), fn(row_angle)
            for r in range(grid_rows):
                table[r * GRID_W : (r + 1) * GRID_W, :] = jnp.where(
                    by_row, rows[r : r + 1, :], cols
                )

    def qkv():
        step = min(256, tokens)
        lanes = iota((1, pair), 1)
        low = lax.rem(lanes, HEAD_DIM) < HEAD_DIM // 2
        ones = one_zero(
            lax.rem(iota((2 * pair, pair), 0), pair) // HEAD_DIM
            == iota((2 * pair, pair), 1) // HEAD_DIM
        )
        gain_q = jnp.concatenate([q_gain[...]] * (pair // HEAD_DIM), axis=1)
        gain_k = jnp.concatenate([k_gain[...]] * (pair // HEAD_DIM), axis=1)

        def turned(x, gain, rows):
            square = x * x
            high = square.astype(bf16)
            rest = (square - high.astype(f32)).astype(bf16)
            mean = dot(jnp.concatenate([high, rest], axis=1), ones) * (1.0 / HEAD_DIM)
            scaled = x * lax.rsqrt(mean + EPSILON) * gain
            swapped = jnp.where(
                low,
                -pltpu.roll(scaled, pair - HEAD_DIM // 2, 1),
                pltpu.roll(scaled, HEAD_DIM // 2, 1),
            )
            return scaled * ctab[rows, :] + swapped * stab[rows, :]

        def body(i, carry):
            rows = pl.ds(pl.multiple_of(i * step, step), step)
            x = dot(xa[rows, :], wqkv[...])
            for g in range(q_cols // pair):
                span = slice(g * pair, (g + 1) * pair)
                q_s[rows, span] = (
                    turned(x[:, span], gain_q, rows) * HEAD_DIM ** (-0.5)
                ).astype(bf16)
            for g in range(kw // pair):
                span = slice(g * pair, (g + 1) * pair)
                k_span = slice(q_cols + g * pair, q_cols + (g + 1) * pair)
                kv[rows, span] = turned(x[:, k_span], gain_k, rows).astype(bf16)
            kv[rows, kw : 2 * kw] = x[:, q_cols + kw :].astype(bf16)
            return carry

        lax.fori_loop(0, tokens // step, body, 0)

    def expand(src, start, rows):
        block = jnp.concatenate([src[:, 0:kw], src[:, kw : 2 * kw]], axis=0)
        source = iota((kw, kv_local * pair), 0)
        column = iota((kw, kv_local * pair), 1)
        spread = one_zero(source == column // pair * HEAD_DIM + lax.rem(column, HEAD_DIM))
        doubled = dot(block, spread).astype(bf16)
        for h in range(kv_local):
            span = slice(h * pair, (h + 1) * pair)
            kd[h, start : start + rows, :] = doubled[0:rows, span]
            ve[h, start : start + rows, 0:pair] = doubled[rows:, span]
            ve[h, start : start + rows, pair : 2 * pair] = jnp.ones((rows, pair), bf16)

    def blank(start):
        for h in range(kv_local):
            kd[h, start : start + WINDOW, :] = jnp.zeros((WINDOW, pair), bf16)
            ve[h, start : start + WINDOW, :] = jnp.zeros((WINDOW, 2 * pair), bf16)

    def halo_start():
        @pl.when(me < n_ep - 1)
        def _():
            halo_up().start()

        @pl.when(me > 0)
        def _():
            halo_down().start()

    def halo_finish():
        @pl.when(me > 0)
        def _():
            halo_up().wait_recv()
            expand(halo.at[0], 0, WINDOW)

        @pl.when(me == 0)
        def _():
            blank(0)

        @pl.when(me < n_ep - 1)
        def _():
            halo_down().wait_recv()
            expand(halo.at[1], WINDOW + tokens, WINDOW)

        @pl.when(me == n_ep - 1)
        def _():
            blank(WINDOW + tokens)

    def attend(first, count, stride):
        span = 3 * WINDOW
        lanes = iota((1, pair), 1)
        left = one_zero(lanes < HEAD_DIM)
        right = one_zero(lanes >= HEAD_DIM)
        query = lax.rem(iota((2 * WINDOW, span), 0), WINDOW)
        key = iota((2 * WINDOW, span), 1)
        seen = (key >= query) & (key <= query + 2 * WINDOW)

        def body(j, carry):
            start = pl.multiple_of((first + stride * j) * WINDOW, WINDOW)
            rows = pl.ds(start, WINDOW)
            keys = pl.ds(start, span)
            for h in range(kv_local):
                cols = slice(h * pair, (h + 1) * pair)
                heads = q_s[rows, cols]
                stacked = jnp.concatenate([heads * left, heads * right], axis=0)
                scores = dot_nt(stacked, kd[h, keys, :])
                weights = jnp.where(seen, jnp.exp(scores), 0.0).astype(bf16)
                mixed = dot(weights, ve[h, keys, :])
                sink_0 = jnp.exp(jnp.full((1, pair), sink[2 * h], f32))
                sink_1 = jnp.exp(jnp.full((1, pair), sink[2 * h + 1], f32))
                upper = mixed[0:WINDOW, 0:pair] / (mixed[0:WINDOW, pair:] + sink_0)
                lower = mixed[WINDOW:, 0:pair] / (mixed[WINDOW:, pair:] + sink_1)
                att[rows, cols] = jnp.where(lanes < HEAD_DIM, upper, lower).astype(bf16)
            return carry

        lax.fori_loop(0, count, body, 0)

    def project():
        tile = 2 * pair
        quarter = attn_ref.shape[1]

        def body(n, carry):
            cols = pl.ds(pl.multiple_of(n * tile, tile), tile)
            x = dot(att[...], wo[:, cols]).astype(bf16)
            for s in range(attn_ref.shape[0]):
                attn_ref[s, :, cols] = x[s * quarter : (s + 1) * quarter]
            return carry

        lax.fori_loop(0, wo.shape[1] // tile, body, 0)
        attn_core(0).start()
        attn_core(1).start()

    def attn_sum():
        attn_core(0).wait_recv()
        attn_core(1).wait_recv()

    def attn_cross(c):
        rows = slice(c * chunk_rows, (c + 1) * chunk_rows)
        attn_y_out[c] = (
            attn_ref[2 * other_side + core, rows].astype(f32)
            + attn_in[other_side, rows].astype(f32)
        ).astype(bf16)
        attn_side(c).start()

    def attn_final(c):
        rows = slice(c * chunk_rows, (c + 1) * chunk_rows)
        attn_side(c).wait_recv()
        attn_out_ref[rows] = (
            attn_ref[2 * side + core, rows].astype(f32)
            + attn_in[side, rows].astype(f32)
            + attn_y_in[c].astype(f32)
        ).astype(bf16)

    nb = tokens // WINDOW

    loads[8].wait()
    plan()
    for i, copy in enumerate(pieces):
        copy.wait()
        if i == XE_PIECES - 1:
            for load in loads[0:8]:
                load.start()
        rms_inplace(xe, i * first_rows, first_rows, e_gain)
    pl.semaphore_wait(barrier, n_ep + 1)

    def load_ffn():
        for copy in loads[0:3]:
            copy.wait()

    def front_norm():
        loads[3].wait()
        rms_inplace(xa, 0, tokens, a_gain)

    def front_qkv():
        for copy in loads[4:8]:
            copy.wait()
        rope_tables()
        qkv()

    if n_ep == 8:
        D(1, True)
        D(4, False)
        D(2, True)
        L0()
        front_norm()
        front_qkv()
        halo_start()
        expand(kv, WINDOW, tokens)
        D(6, False)
        load_ffn()
        C(0)
        D(5, False)
        A(1, True)
        Z(1)
        attend(1, nb - 2, 1)
        E(0)
        C(1)
        A(4, False)
        build_mix()
        A(2, True)
        Z(2)
        C(2)
        D(7, False)
        E(1)
        D(3, True)
        halo_finish()
        attend(0, 2, nb - 1)
        E(2)
        B(4)
        project()
        A(6, False)
        attn_sum()
        C(4)
        E(4)
        F(0, True)
        B(6)
        A(5, False)
        C(6)
        attn_cross(0)
        E(6)
        F(4, False)
        A(3, True)
        Z(3)
        F(2, False)
        A(7, False)
        attn_cross(4)
        F(1, False)
        B(5)
        C(5)
        F(6, False)
        C(3)
        attn_final(0)
        E(5)
        attn_cross(7)
        B(7)
        G(1)
        C(7)
        G(4)
        attn_cross(2)
        attn_final(4)
        E(7)
        F(5, False)
        G(2)
        F(7, False)
        E(3)
        attn_cross(3)
        attn_cross(6)
        attn_cross(1)
        F(3, False)
        G(6)
        G(5)
        attn_final(3)
        attn_final(2)
        attn_cross(5)
        G(7)
        attn_final(5)
        attn_final(6)
        attn_final(7)
        attn_final(1)
        G(3)
    else:
        def each(low, high, fn):
            def body(k, carry):
                fn(k)
                return carry

            lax.fori_loop(low, high, body, 0)

        each(half, n_ep, lambda k: D(k, False))
        each(1, half, lambda k: D(k, True))
        L0()
        load_ffn()
        front_norm()
        front_qkv()
        halo_start()
        expand(kv, WINDOW, tokens)
        attend(1, nb - 2, 1)
        each(1, half, lambda k: A(k, True))
        each(1, half, Z)
        each(half, n_ep, lambda k: A(k, False))
        halo_finish()
        attend(0, 2, nb - 1)
        project()
        build_mix()
        each(half, n_ep, B)
        each(0, n_ep, C)
        each(0, n_ep, E)
        attn_sum()
        F(0, True)
        each(1, n_ep, lambda k: F(k, False))
        for c in range(ATTN_CHUNKS):
            attn_cross(c)
        each(1, n_ep, G)
        for c in range(ATTN_CHUNKS):
            attn_final(c)

    out_ref[...] = total[...].astype(bf16)

    def drain(k, carry):
        @pl.when(k > 0)
        def _():
            dispatch(k).wait_send()
            give_back(k).wait_send()

        to_partner(k).wait_send()

        @pl.when(k >= half)
        def _():
            to_across(k).wait_send()

        @pl.when((k > 0) & (k < half))
        def _():
            dispatch_other(k).wait_send()

        relay(k).wait_send()
        sum_core(k).wait_send()
        sum_side(k).wait_send()
        return carry

    lax.fori_loop(0, n_ep, drain, 0)
    attn_core(0).wait_send()
    attn_core(1).wait_send()
    for c in range(ATTN_CHUNKS):
        attn_side(c).wait_send()

    @pl.when(me < n_ep - 1)
    def _():
        halo_up().wait_send()

    @pl.when(me > 0)
    def _():
        halo_down().wait_send()


def per_device(
    x_attend, attend_gain, w_query, w_key, w_value, query_gain, key_gain, sink_logit, w_output,
    x_experts, expert_gain, routes, group_prob, expert_prob, w_gate, w_up, w_down,
):
    tokens, model_width = x_attend.shape
    q_cols, kv_cols = w_query.shape[1], w_key.shape[1]
    kv_local = kv_cols // HEAD_DIM
    tp_count, n_ep = lax.axis_size("tp"), lax.axis_size("ep")
    moe_rows, top_count = routes.shape
    capacity = max(2, (3 * moe_rows * top_count + 2 * n_ep - 1) // (2 * n_ep))
    col_width = model_width // tp_count
    hidden_cols = w_gate.shape[2]
    slice_rows = tokens // tp_count
    ext = tokens + 2 * WINDOW
    pair = 2 * HEAD_DIM
    chunk = slice_rows // ATTN_CHUNKS
    vmem = pl.BlockSpec(memory_space=pltpu.VMEM)
    smem = pl.BlockSpec(memory_space=pltpu.SMEM)
    hbm = pl.BlockSpec(memory_space=pl.ANY)
    dma = pltpu.SemaphoreType.DMA

    def buf(*shape, dtype=bf16):
        return pltpu.VMEM(shape, dtype)

    expert_out, attend_out = pl.pallas_call(
        functools.partial(fused_kernel, n_ep),
        out_shape=(buf(moe_rows, col_width), buf(slice_rows, model_width)),
        in_specs=[
            hbm, vmem, hbm, hbm, hbm, vmem, vmem, smem, hbm,
            hbm, vmem, vmem, hbm, vmem, hbm, hbm, hbm,
        ],
        out_specs=(vmem, vmem),
        scratch_shapes=[
            buf(tokens, model_width),
            buf(model_width, q_cols + 2 * kv_cols),
            buf(q_cols, model_width),
            buf(moe_rows, model_width),
            buf(model_width, 2 * hidden_cols),
            buf(hidden_cols, model_width),
            buf(tokens, pair, dtype=f32),
            buf(tokens, pair, dtype=f32),
            buf(tokens, q_cols),
            buf(tokens, 2 * kv_cols),
            buf(2, WINDOW, 2 * kv_cols),
            buf(kv_local, ext, pair),
            buf(kv_local, ext, 2 * pair),
            buf(tokens, q_cols),
            buf(tp_count, slice_rows, model_width),
            buf(2, slice_rows, model_width),
            buf(ATTN_CHUNKS, chunk, model_width),
            buf(ATTN_CHUNKS, chunk, model_width),
            buf(1, moe_rows, dtype=f32),
            buf(n_ep, moe_rows, dtype=f32),
            buf(moe_rows, n_ep, dtype=f32),
            buf(moe_rows, n_ep, dtype=f32),
            buf(n_ep, moe_rows, capacity),
            buf(n_ep, capacity, col_width),
            buf(n_ep // 2, capacity, col_width),
            buf(tp_count, n_ep, capacity, col_width),
            buf(n_ep, 2, capacity, col_width),
            buf(n_ep, 2, capacity, col_width),
            buf(n_ep, 2, capacity, col_width),
            buf(n_ep, capacity, col_width),
            buf(n_ep, capacity, col_width, dtype=f32),
            buf(n_ep, capacity, col_width),
            buf(n_ep, capacity, col_width),
            buf(n_ep, capacity, col_width),
            buf(moe_rows, col_width, dtype=f32),
            dma((9,)),
            dma((XE_PIECES,)),
        ]
        + [dma((n_ep,))] * 16
        + [dma((2,))] * 2
        + [dma((ATTN_CHUNKS,))] * 2
        + [dma((2,))] * 2,
        compiler_params=pltpu.CompilerParams(
            collective_id=0, has_side_effects=True, vmem_limit_bytes=60 * 1024 * 1024
        ),
    )(
        x_attend, attend_gain[None], w_query, w_key, w_value, query_gain[None], key_gain[None],
        sink_logit, w_output, x_experts, expert_gain[None], routes.T, group_prob,
        expert_prob.T, w_gate[0], w_up[0], w_down[0],
    )
    return (attend_out, expert_out)


def solution(mesh):
    placed = (
        P("ep", None),
        P(),
        P(None, "tp"),
        P(None, "tp"),
        P(None, "tp"),
        P(),
        P(),
        P("tp"),
        P("tp", None),
        P("ep", None),
        P(),
        P("ep", None),
        P("ep"),
        P("ep", None),
        P("ep", None, "tp"),
        P("ep", None, "tp"),
        P("ep", "tp", None),
    )
    return jax.shard_map(
        per_device,
        mesh=mesh,
        in_specs=placed,
        out_specs=(P(("ep", "tp"), None), P("ep", "tp")),
        check_vma=False,
    )
```

```python
import functools

import jax
import jax.numpy as jnp
from jax import lax
from jax.experimental import pallas as pl
from jax.experimental.pallas import tpu as pltpu
from jax.sharding import PartitionSpec as P

HEAD_DIM = 64
WINDOW = 128
GRID_W = 64
MESH = pl.DeviceIdType.MESH
EPSILON = 1e-06
LOG_BASE = 9.210340371976184
ATTN_CHUNKS = 8
XE_PIECES = 3
bf16, f32, i32 = jnp.bfloat16, jnp.float32, jnp.int32


def flip(a, b, count):
    total, bit = 0, 1
    while bit < count:
        total = total + lax.rem(a // bit + b // bit, 2) * bit
        bit *= 2
    return total


def iota(shape, dim):
    return lax.broadcasted_iota(i32, shape, dim)


def dot(a, b):
    return jnp.dot(a, b, preferred_element_type=f32)


def dot_nt(a, b):
    return lax.dot_general(a, b, (((1,), (1,)), ((), ())), preferred_element_type=f32)


def one_zero(mask):
    return jnp.where(mask, 1.0, 0.0).astype(bf16)


def rms_inplace(ref, first, count, gain_ref):
    chunk, lanes = 64, 128
    features = ref.shape[1]
    steps = 2 if count % (2 * chunk) == 0 else 1

    def body(i, carry):
        for j in range(steps):
            start = first + (i * steps + j) * chunk
            rows = pl.ds(pl.multiple_of(start, chunk), chunk)
            v = ref[rows, :].astype(f32)
            square = v * v
            part = square[:, 0:lanes]
            for c in range(lanes, features, lanes):
                part = part + square[:, c : c + lanes]
            mean = jnp.sum(part, axis=-1, keepdims=True) * (1.0 / features)
            ref[rows, :] = (v * lax.rsqrt(mean + EPSILON) * gain_ref[...]).astype(bf16)
        return carry

    lax.fori_loop(0, count // (chunk * steps), body, 0)


def fused_kernel(
    n_ep,
    xa_hbm, a_gain_hbm, wq_hbm, wk_hbm, wv_hbm, q_gain_hbm, k_gain_hbm, sink_hbm, wo_hbm,
    xe_hbm, e_gain_hbm, routes_hbm, group_hbm, expert_hbm, wg_hbm, wu_hbm, wd_hbm,
    out_ref, attn_out_ref,
    xa, wqkv, wo, xe, wgu, wd,
    ctab, stab, q_s, kv, halo, kd, ve, att,
    attn_ref, attn_in, attn_y_out, attn_y_in,
    a_gain, q_gain, k_gain, sink, e_gain, routes_t, expert_p,
    group_p, rank_s, rank_tn, share_tn, mix,
    send_own, send_other, rows_buf, part_out, part_keep, part_in,
    y_out, y_own, y_in, final, back, total,
    l_sem, x_sem, s_sem,
    d_send, d_recv, e_send, e_recv, p_send, p_recv, y_send, y_recv,
    r_send, r_recv, c_send, c_recv, s_send, s_recv, f_send, f_recv,
    a_send, a_recv, b_send, b_recv, h_send, h_recv,
):
    me = lax.axis_index("ep")
    lane = lax.axis_index("tp")
    core = lax.rem(lane, 2)
    side = lane // 2
    other_core, other_side = 1 - core, 1 - side
    partner = 2 * side + other_core
    across = 2 * other_side + core
    capacity, width = send_own.shape[1:]
    half = n_ep // 2
    tokens = xa.shape[0]
    moe_tokens = xe.shape[0]
    kv_local, ext_rows, pair = kd.shape
    q_cols = q_s.shape[1]
    hidden_cols = wd.shape[0]

    def local(i, src, dst):
        return pltpu.make_async_copy(src, dst, l_sem.at[i])

    kw = wk_hbm.shape[1]
    loads = [
        local(0, wg_hbm, wgu.at[:, 0:hidden_cols]),
        local(1, wu_hbm, wgu.at[:, hidden_cols : 2 * hidden_cols]),
        local(2, wd_hbm, wd),
        local(3, xa_hbm, xa),
        local(4, wq_hbm, wqkv.at[:, 0:q_cols]),
        local(5, wk_hbm, wqkv.at[:, q_cols : q_cols + kw]),
        local(6, wv_hbm, wqkv.at[:, q_cols + kw : q_cols + 2 * kw]),
        local(7, wo_hbm, wo),
    ]
    small = [
        pltpu.make_async_copy(src, dst, s_sem.at[i])
        for i, (src, dst) in enumerate(
            [
                (routes_hbm, routes_t),
                (expert_hbm, expert_p),
                (group_hbm, group_p.at[0]),
                (e_gain_hbm, e_gain.at[0]),
                (a_gain_hbm, a_gain.at[0]),
                (q_gain_hbm, q_gain.at[0]),
                (k_gain_hbm, k_gain.at[0]),
                (sink_hbm, sink),
            ]
        )
    ]
    for copy in small:
        copy.start()
    first_rows = moe_tokens // XE_PIECES
    pieces = [
        pltpu.make_async_copy(
            xe_hbm.at[i * first_rows : (i + 1) * first_rows],
            xe.at[i * first_rows : (i + 1) * first_rows],
            x_sem.at[i],
        )
        for i in range(XE_PIECES)
    ]
    for copy in pieces:
        copy.start()

    barrier = pltpu.get_barrier_semaphore()

    def greet(k, carry):
        pl.semaphore_signal(
            barrier, inc=1, device_id={"ep": flip(me, k, n_ep), "tp": lane}, device_id_type=MESH
        )
        return carry

    lax.fori_loop(1, n_ep, greet, 0)
    for peer in (partner, across):
        pl.semaphore_signal(barrier, inc=1, device_id={"ep": me, "tp": peer}, device_id_type=MESH)

    def remote(src, dst, sends, recvs, k, ep, tp):
        return pltpu.make_async_remote_copy(
            src_ref=src,
            dst_ref=dst,
            send_sem=sends.at[k],
            recv_sem=recvs.at[k],
            device_id={"ep": ep, "tp": tp},
            device_id_type=MESH,
        )

    def dispatch(k):
        dest = flip(me, k, n_ep)
        return remote(send_own.at[k], rows_buf.at[lane, k], d_send, d_recv, k, dest, lane)

    def dispatch_other(k):
        dest = flip(me, k, n_ep)
        return remote(send_other.at[k], rows_buf.at[across, k], e_send, e_recv, k, dest, lane)

    def to_partner(k):
        block = rows_buf.at[lane, k]
        return remote(block, block, p_send, p_recv, k, me, partner)

    def to_across(k):
        block = rows_buf.at[lane, k]
        return remote(block, block, y_send, y_recv, k, me, across)

    def relay(k):
        block = rows_buf.at[across, k]
        return remote(block, block, r_send, r_recv, k, me, partner)

    def sum_core(k):
        return remote(part_out.at[k], part_in.at[k], c_send, c_recv, k, me, partner)

    def sum_side(k):
        return remote(y_out.at[k], y_in.at[k], s_send, s_recv, k, me, across)

    def give_back(k):
        return remote(final.at[k], back.at[k], f_send, f_recv, k, flip(me, k, n_ep), lane)

    def attn_core(s):
        return remote(
            attn_ref.at[2 * s + other_core], attn_in.at[s], a_send, a_recv, s, me, partner
        )

    chunk_rows = attn_y_out.shape[1]

    def attn_side(c):
        return remote(attn_y_out.at[c], attn_y_in.at[c], b_send, b_recv, c, me, across)

    def halo_up():
        return remote(
            kv.at[tokens - WINDOW : tokens], halo.at[0], h_send, h_recv, 0, me + 1, lane
        )

    def halo_down():
        return remote(kv.at[0:WINDOW], halo.at[1], h_send, h_recv, 1, me - 1, lane)

    def plan():
        names = iota((n_ep, moe_tokens), 0)
        named = None
        share = jnp.zeros((n_ep, moe_tokens), f32)
        top = routes_t.shape[0]
        prob_sum = expert_p[0:1, :]
        for j in range(1, top):
            prob_sum = prob_sum + expert_p[j : j + 1, :]
        for j in range(top):
            chosen = routes_t[j : j + 1, :] == names
            weight = group_p[...] * expert_p[j : j + 1, :] / prob_sum
            share = share + jnp.where(chosen, weight, 0.0)
            named = chosen if named is None else named | chosen
        before = one_zero(iota((moe_tokens, moe_tokens), 0) < iota((moe_tokens, moe_tokens), 1))
        same = one_zero(iota((moe_tokens, moe_tokens), 0) == iota((moe_tokens, moe_tokens), 1))
        rank = jnp.where(named, dot(one_zero(named), before), -1.0)
        rank_s[...] = rank
        rank_tn[...] = dot_nt(same, rank.astype(bf16))
        share_tn[...] = dot_nt(same, share.astype(bf16))

    def pick(k):
        row = rank_s[pl.ds(flip(me, k, n_ep), 1), :]
        return one_zero(row == iota((capacity, moe_tokens), 0).astype(f32))

    def gathered(chosen, quarter):
        start = pl.multiple_of(quarter * width, width)
        return dot(chosen, xe[:, pl.ds(start, width)]).astype(bf16)

    def D(k, near):
        chosen = pick(k)
        send_own[k] = gathered(chosen, lane)
        dispatch(k).start()
        if near:
            send_other[k] = gathered(chosen, across)
            dispatch_other(k).start()

    def L0():
        chosen = pick(0)
        rows_buf[lane, 0] = gathered(chosen, lane)
        to_partner(0).start()
        rows_buf[across, 0] = gathered(chosen, across)
        relay(0).start()

    def build_mix():
        columns = iota((moe_tokens, n_ep), 1)
        slots = iota((moe_tokens, capacity), 1).astype(f32)

        def body(e, carry):
            rank = jnp.sum(jnp.where(columns == e, rank_tn[...], 0.0), axis=1, keepdims=True)
            share = jnp.sum(jnp.where(columns == e, share_tn[...], 0.0), axis=1, keepdims=True)
            mix[e] = jnp.where(rank == slots, share, 0.0).astype(bf16)
            return carry

        lax.fori_loop(0, n_ep, body, 0)

    def A(k, near):
        dispatch(k).wait_recv()
        if not near:
            to_across(k).start()
        to_partner(k).start()

    def Z(k):
        dispatch_other(k).wait_recv()
        relay(k).start()

    def B(k):
        to_across(k).wait_recv()
        relay(k).start()

    def C(k):
        to_partner(k).wait_recv()
        relay(k).wait_recv()
        rows = jnp.concatenate([rows_buf[q, k] for q in range(4)], axis=1)
        acts = dot(rows, wgu[...])
        gate, up = acts[:, 0:hidden_cols], acts[:, hidden_cols:]
        hidden = (gate / (1.0 + jnp.exp(-gate)) * up).astype(bf16)
        for c, target in ((other_core, part_out), (core, part_keep)):
            for s in range(2):
                start = pl.multiple_of((2 * s + c) * width, width)
                target[k, s] = dot(hidden, wd[:, pl.ds(start, width)]).astype(bf16)
            if target is part_out:
                sum_core(k).start()

    def E(k):
        sum_core(k).wait_recv()
        y_out[k] = (
            part_keep[k, other_side].astype(f32) + part_in[k, other_side].astype(f32)
        ).astype(bf16)
        sum_side(k).start()
        y_own[k] = part_keep[k, side].astype(f32) + part_in[k, side].astype(f32)

    def F(k, own):
        sum_side(k).wait_recv()
        final[k] = (y_own[k] + y_in[k].astype(f32)).astype(bf16)
        if own:
            total[...] = dot(mix[me], final[0])
        else:
            give_back(k).start()

    def G(k):
        give_back(k).wait_recv()
        total[...] += dot(mix[flip(me, k, n_ep)], back[k])

    def rope_tables():
        lanes = lax.rem(iota((GRID_W, pair), 1), HEAD_DIM // 2)
        quarter = HEAD_DIM // 4
        inverse = jnp.exp(lax.rem(lanes, quarter).astype(f32) * (-LOG_BASE / quarter))
        by_row = lanes < quarter
        grid_rows = tokens // GRID_W
        first = me * grid_rows
        col_angle = iota((GRID_W, pair), 0).astype(f32) * inverse
        row_angle = (iota((grid_rows, pair), 0) + first).astype(f32) * inverse[0:grid_rows]
        for table, fn in ((ctab, jnp.cos), (stab, jnp.sin)):
            cols, rows = fn(col_angle), fn(row_angle)
            for r in range(grid_rows):
                table[r * GRID_W : (r + 1) * GRID_W, :] = jnp.where(
                    by_row, rows[r : r + 1, :], cols
                )

    def qkv():
        step = min(256, tokens)
        lanes = iota((1, pair), 1)
        low = lax.rem(lanes, HEAD_DIM) < HEAD_DIM // 2
        ones = one_zero(
            lax.rem(iota((2 * pair, pair), 0), pair) // HEAD_DIM
            == iota((2 * pair, pair), 1) // HEAD_DIM
        )
        gain_q = jnp.concatenate([q_gain[...]] * (pair // HEAD_DIM), axis=1)
        gain_k = jnp.concatenate([k_gain[...]] * (pair // HEAD_DIM), axis=1)

        def turned(x, gain, rows):
            square = x * x
            high = square.astype(bf16)
            rest = (square - high.astype(f32)).astype(bf16)
            mean = dot(jnp.concatenate([high, rest], axis=1), ones) * (1.0 / HEAD_DIM)
            scaled = x * lax.rsqrt(mean + EPSILON) * gain
            swapped = jnp.where(
                low,
                -pltpu.roll(scaled, pair - HEAD_DIM // 2, 1),
                pltpu.roll(scaled, HEAD_DIM // 2, 1),
            )
            return scaled * ctab[rows, :] + swapped * stab[rows, :]

        def body(i, carry):
            rows = pl.ds(pl.multiple_of(i * step, step), step)
            x = dot(xa[rows, :], wqkv[...])
            for g in range(q_cols // pair):
                span = slice(g * pair, (g + 1) * pair)
                q_s[rows, span] = (
                    turned(x[:, span], gain_q, rows) * HEAD_DIM ** (-0.5)
                ).astype(bf16)
            for g in range(kw // pair):
                span = slice(g * pair, (g + 1) * pair)
                k_span = slice(q_cols + g * pair, q_cols + (g + 1) * pair)
                kv[rows, span] = turned(x[:, k_span], gain_k, rows).astype(bf16)
            kv[rows, kw : 2 * kw] = x[:, q_cols + kw :].astype(bf16)
            return carry

        lax.fori_loop(0, tokens // step, body, 0)

    def expand(src, start, rows):
        block = jnp.concatenate([src[:, 0:kw], src[:, kw : 2 * kw]], axis=0)
        source = iota((kw, kv_local * pair), 0)
        column = iota((kw, kv_local * pair), 1)
        spread = one_zero(source == column // pair * HEAD_DIM + lax.rem(column, HEAD_DIM))
        doubled = dot(block, spread).astype(bf16)
        for h in range(kv_local):
            span = slice(h * pair, (h + 1) * pair)
            kd[h, start : start + rows, :] = doubled[0:rows, span]
            ve[h, start : start + rows, 0:pair] = doubled[rows:, span]
            ve[h, start : start + rows, pair : 2 * pair] = jnp.ones((rows, pair), bf16)

    def blank(start):
        for h in range(kv_local):
            kd[h, start : start + WINDOW, :] = jnp.zeros((WINDOW, pair), bf16)
            ve[h, start : start + WINDOW, :] = jnp.zeros((WINDOW, 2 * pair), bf16)

    def halo_start():
        @pl.when(me < n_ep - 1)
        def _():
            halo_up().start()

        @pl.when(me > 0)
        def _():
            halo_down().start()

    def halo_finish():
        @pl.when(me > 0)
        def _():
            halo_up().wait_recv()
            expand(halo.at[0], 0, WINDOW)

        @pl.when(me == 0)
        def _():
            blank(0)

        @pl.when(me < n_ep - 1)
        def _():
            halo_down().wait_recv()
            expand(halo.at[1], WINDOW + tokens, WINDOW)

        @pl.when(me == n_ep - 1)
        def _():
            blank(WINDOW + tokens)

    def attend(first, count, stride):
        span = 3 * WINDOW
        lanes = iota((1, pair), 1)
        left = one_zero(lanes < HEAD_DIM)
        right = one_zero(lanes >= HEAD_DIM)
        query = lax.rem(iota((2 * WINDOW, span), 0), WINDOW)
        key = iota((2 * WINDOW, span), 1)
        seen = (key >= query) & (key <= query + 2 * WINDOW)

        def body(j, carry):
            start = pl.multiple_of((first + stride * j) * WINDOW, WINDOW)
            rows = pl.ds(start, WINDOW)
            keys = pl.ds(start, span)
            for h in range(kv_local):
                cols = slice(h * pair, (h + 1) * pair)
                heads = q_s[rows, cols]
                stacked = jnp.concatenate([heads * left, heads * right], axis=0)
                scores = dot_nt(stacked, kd[h, keys, :])
                weights = jnp.where(seen, jnp.exp(scores), 0.0).astype(bf16)
                mixed = dot(weights, ve[h, keys, :])
                sink_0 = jnp.exp(jnp.full((1, pair), sink[2 * h], f32))
                sink_1 = jnp.exp(jnp.full((1, pair), sink[2 * h + 1], f32))
                upper = mixed[0:WINDOW, 0:pair] / (mixed[0:WINDOW, pair:] + sink_0)
                lower = mixed[WINDOW:, 0:pair] / (mixed[WINDOW:, pair:] + sink_1)
                att[rows, cols] = jnp.where(lanes < HEAD_DIM, upper, lower).astype(bf16)
            return carry

        lax.fori_loop(0, count, body, 0)

    def project():
        tile = 2 * pair
        quarter = attn_ref.shape[1]

        def body(n, carry):
            cols = pl.ds(pl.multiple_of(n * tile, tile), tile)
            x = dot(att[...], wo[:, cols]).astype(bf16)
            for s in range(attn_ref.shape[0]):
                attn_ref[s, :, cols] = x[s * quarter : (s + 1) * quarter]
            return carry

        lax.fori_loop(0, wo.shape[1] // tile, body, 0)
        attn_core(0).start()
        attn_core(1).start()

    def attn_sum():
        attn_core(0).wait_recv()
        attn_core(1).wait_recv()

    def attn_cross(c):
        rows = slice(c * chunk_rows, (c + 1) * chunk_rows)
        attn_y_out[c] = (
            attn_ref[2 * other_side + core, rows].astype(f32)
            + attn_in[other_side, rows].astype(f32)
        ).astype(bf16)
        attn_side(c).start()

    def attn_final(c):
        rows = slice(c * chunk_rows, (c + 1) * chunk_rows)
        attn_side(c).wait_recv()
        attn_out_ref[rows] = (
            attn_ref[2 * side + core, rows].astype(f32)
            + attn_in[side, rows].astype(f32)
            + attn_y_in[c].astype(f32)
        ).astype(bf16)

    nb = tokens // WINDOW

    for copy in small[0:4]:
        copy.wait()
    plan()
    for i, copy in enumerate(pieces):
        copy.wait()
        if i == XE_PIECES - 1:
            for load in loads[0:8]:
                load.start()
        rms_inplace(xe, i * first_rows, first_rows, e_gain)
    pl.semaphore_wait(barrier, n_ep + 1)

    def load_ffn():
        for copy in loads[0:3]:
            copy.wait()

    def front_norm():
        for copy in small[4:8]:
            copy.wait()
        loads[3].wait()
        rms_inplace(xa, 0, tokens, a_gain)

    def front_qkv():
        for copy in loads[4:8]:
            copy.wait()
        rope_tables()
        qkv()

    if n_ep == 8:
        D(6, False)
        L0()
        D(1, True)
        D(4, False)
        front_norm()
        D(2, True)
        D(7, False)
        load_ffn()
        C(0)
        front_qkv()
        A(6, False)
        build_mix()
        E(0)
        halo_start()
        B(6)
        A(4, False)
        Z(1)
        Z(2)
        A(2, True)
        C(6)
        F(0, True)
        E(6)
        B(4)
        D(5, False)
        D(3, True)
        C(2)
        A(7, False)
        A(1, True)
        C(4)
        E(2)
        halo_finish()
        expand(kv, WINDOW, tokens)
        F(6, False)
        E(4)
        attend(0, 2, nb - 1)
        attend(1, nb - 2, 1)
        C(1)
        B(7)
        project()
        A(5, False)
        A(3, True)
        C(7)
        E(1)
        E(7)
        F(4, False)
        B(5)
        G(6)
        attn_sum()
        F(2, False)
        Z(3)
        C(5)
        attn_cross(1)
        C(3)
        F(1, False)
        attn_cross(6)
        E(5)
        F(7, False)
        E(3)
        attn_cross(0)
        G(2)
        attn_final(1)
        attn_cross(2)
        F(5, False)
        attn_cross(4)
        F(3, False)
        attn_cross(3)
        attn_cross(5)
        attn_final(0)
        G(4)
        G(1)
        attn_cross(7)
        attn_final(5)
        attn_final(6)
        attn_final(4)
        G(7)
        attn_final(2)
        G(5)
        attn_final(3)
        G(3)
        attn_final(7)
    else:
        def each(low, high, fn):
            def body(k, carry):
                fn(k)
                return carry

            lax.fori_loop(low, high, body, 0)

        each(half, n_ep, lambda k: D(k, False))
        each(1, half, lambda k: D(k, True))
        L0()
        load_ffn()
        front_norm()
        front_qkv()
        halo_start()
        expand(kv, WINDOW, tokens)
        attend(1, nb - 2, 1)
        each(1, half, lambda k: A(k, True))
        each(1, half, Z)
        each(half, n_ep, lambda k: A(k, False))
        halo_finish()
        attend(0, 2, nb - 1)
        project()
        build_mix()
        each(half, n_ep, B)
        each(0, n_ep, C)
        each(0, n_ep, E)
        attn_sum()
        F(0, True)
        each(1, n_ep, lambda k: F(k, False))
        for c in range(ATTN_CHUNKS):
            attn_cross(c)
        each(1, n_ep, G)
        for c in range(ATTN_CHUNKS):
            attn_final(c)

    out_ref[...] = total[...].astype(bf16)

    def drain(k, carry):
        @pl.when(k > 0)
        def _():
            dispatch(k).wait_send()
            give_back(k).wait_send()

        to_partner(k).wait_send()

        @pl.when(k >= half)
        def _():
            to_across(k).wait_send()

        @pl.when((k > 0) & (k < half))
        def _():
            dispatch_other(k).wait_send()

        relay(k).wait_send()
        sum_core(k).wait_send()
        sum_side(k).wait_send()
        return carry

    lax.fori_loop(0, n_ep, drain, 0)
    attn_core(0).wait_send()
    attn_core(1).wait_send()
    for c in range(ATTN_CHUNKS):
        attn_side(c).wait_send()

    @pl.when(me < n_ep - 1)
    def _():
        halo_up().wait_send()

    @pl.when(me > 0)
    def _():
        halo_down().wait_send()


def per_device(
    x_attend, attend_gain, w_query, w_key, w_value, query_gain, key_gain, sink_logit, w_output,
    x_experts, expert_gain, routes, group_prob, expert_prob, w_gate, w_up, w_down,
):
    tokens, model_width = x_attend.shape
    q_cols, kv_cols = w_query.shape[1], w_key.shape[1]
    kv_local = kv_cols // HEAD_DIM
    tp_count, n_ep = lax.axis_size("tp"), lax.axis_size("ep")
    moe_rows, top_count = routes.shape
    capacity = max(2, (3 * moe_rows * top_count + 2 * n_ep - 1) // (2 * n_ep))
    col_width = model_width // tp_count
    hidden_cols = w_gate.shape[2]
    slice_rows = tokens // tp_count
    ext = tokens + 2 * WINDOW
    pair = 2 * HEAD_DIM
    chunk = slice_rows // ATTN_CHUNKS
    vmem = pl.BlockSpec(memory_space=pltpu.VMEM)
    hbm = pl.BlockSpec(memory_space=pl.ANY)
    dma = pltpu.SemaphoreType.DMA

    def buf(*shape, dtype=bf16):
        return pltpu.VMEM(shape, dtype)

    expert_out, attend_out = pl.pallas_call(
        functools.partial(fused_kernel, n_ep),
        out_shape=(buf(moe_rows, col_width), buf(slice_rows, model_width)),
        in_specs=[hbm] * 17,
        out_specs=(vmem, vmem),
        scratch_shapes=[
            buf(tokens, model_width),
            buf(model_width, q_cols + 2 * kv_cols),
            buf(q_cols, model_width),
            buf(moe_rows, model_width),
            buf(model_width, 2 * hidden_cols),
            buf(hidden_cols, model_width),
            buf(tokens, pair, dtype=f32),
            buf(tokens, pair, dtype=f32),
            buf(tokens, q_cols),
            buf(tokens, 2 * kv_cols),
            buf(2, WINDOW, 2 * kv_cols),
            buf(kv_local, ext, pair),
            buf(kv_local, ext, 2 * pair),
            buf(tokens, q_cols),
            buf(tp_count, slice_rows, model_width),
            buf(2, slice_rows, model_width),
            buf(ATTN_CHUNKS, chunk, model_width),
            buf(ATTN_CHUNKS, chunk, model_width),
            buf(1, model_width, dtype=f32),
            buf(1, HEAD_DIM, dtype=f32),
            buf(1, HEAD_DIM, dtype=f32),
            pltpu.SMEM(sink_logit.shape, f32),
            buf(1, model_width, dtype=f32),
            buf(top_count, moe_rows, dtype=i32),
            buf(top_count, moe_rows, dtype=f32),
            buf(1, moe_rows, dtype=f32),
            buf(n_ep, moe_rows, dtype=f32),
            buf(moe_rows, n_ep, dtype=f32),
            buf(moe_rows, n_ep, dtype=f32),
            buf(n_ep, moe_rows, capacity),
            buf(n_ep, capacity, col_width),
            buf(n_ep // 2, capacity, col_width),
            buf(tp_count, n_ep, capacity, col_width),
            buf(n_ep, 2, capacity, col_width),
            buf(n_ep, 2, capacity, col_width),
            buf(n_ep, 2, capacity, col_width),
            buf(n_ep, capacity, col_width),
            buf(n_ep, capacity, col_width, dtype=f32),
            buf(n_ep, capacity, col_width),
            buf(n_ep, capacity, col_width),
            buf(n_ep, capacity, col_width),
            buf(moe_rows, col_width, dtype=f32),
            dma((8,)),
            dma((XE_PIECES,)),
            dma((8,)),
        ]
        + [dma((n_ep,))] * 16
        + [dma((2,))] * 2
        + [dma((ATTN_CHUNKS,))] * 2
        + [dma((2,))] * 2,
        compiler_params=pltpu.CompilerParams(
            collective_id=0, has_side_effects=True, vmem_limit_bytes=60 * 1024 * 1024
        ),
    )(
        x_attend, attend_gain, w_query, w_key, w_value, query_gain, key_gain,
        sink_logit, w_output, x_experts, expert_gain, routes.T, group_prob,
        expert_prob.T, w_gate[0], w_up[0], w_down[0],
    )
    return (attend_out, expert_out)


def solution(mesh):
    placed = (
        P("ep", None),
        P(),
        P(None, "tp"),
        P(None, "tp"),
        P(None, "tp"),
        P(),
        P(),
        P("tp"),
        P("tp", None),
        P("ep", None),
        P(),
        P("ep", None),
        P("ep"),
        P("ep", None),
        P("ep", None, "tp"),
        P("ep", None, "tp"),
        P("ep", "tp", None),
    )
    return jax.shard_map(
        per_device,
        mesh=mesh,
        in_specs=placed,
        out_specs=(P(("ep", "tp"), None), P("ep", "tp")),
        check_vma=False,
    )
```

```python
import functools

import jax
import jax.numpy as jnp
from jax import lax
from jax.experimental import pallas as pl
from jax.experimental.pallas import tpu as pltpu
from jax.sharding import PartitionSpec as P

HEAD_DIM = 64
WINDOW = 128
GRID_W = 64
MESH = pl.DeviceIdType.MESH
EPSILON = 1e-06
LOG_BASE = 9.210340371976184
ATTN_CHUNKS = 8
XE_PIECES = 3
bf16, f32, i32 = jnp.bfloat16, jnp.float32, jnp.int32


def flip(a, b, count):
    total, bit = 0, 1
    while bit < count:
        total = total + lax.rem(a // bit + b // bit, 2) * bit
        bit *= 2
    return total


def iota(shape, dim):
    return lax.broadcasted_iota(i32, shape, dim)


def dot(a, b):
    return jnp.dot(a, b, preferred_element_type=f32)


def dot_nt(a, b):
    return lax.dot_general(a, b, (((1,), (1,)), ((), ())), preferred_element_type=f32)


def one_zero(mask):
    return jnp.where(mask, 1.0, 0.0).astype(bf16)


def rms_inplace(ref, first, count, gain_ref):
    chunk, lanes = 64, 128
    features = ref.shape[1]
    steps = 2 if count % (2 * chunk) == 0 else 1

    def body(i, carry):
        for j in range(steps):
            start = first + (i * steps + j) * chunk
            rows = pl.ds(pl.multiple_of(start, chunk), chunk)
            v = ref[rows, :].astype(f32)
            square = v * v
            part = square[:, 0:lanes]
            for c in range(lanes, features, lanes):
                part = part + square[:, c : c + lanes]
            mean = jnp.sum(part, axis=-1, keepdims=True) * (1.0 / features)
            ref[rows, :] = (v * lax.rsqrt(mean + EPSILON) * gain_ref[...]).astype(bf16)
        return carry

    lax.fori_loop(0, count // (chunk * steps), body, 0)


def fused_kernel(
    n_ep,
    xa_hbm, a_gain_hbm, wq_hbm, wk_hbm, wv_hbm, q_gain_hbm, k_gain_hbm, sink_hbm, wo_hbm,
    xe_hbm, e_gain_hbm, routes_hbm, group_hbm, expert_hbm, wg_hbm, wu_hbm, wd_hbm,
    out_ref, attn_out_ref,
    xa, wqkv, wo, xe, wgu, wd,
    ctab, stab, q_s, kv, halo, kd, ve, att,
    attn_ref, attn_in, attn_y_out, attn_y_in,
    a_gain, q_gain, k_gain, sink, e_gain, routes_t, expert_p,
    group_p, rank_s, rank_tn, share_tn, mix,
    send_own, send_other, rows_buf, part_out, part_keep, part_in,
    y_out, y_own, y_in, final, back, total,
    l_sem, x_sem, s_sem,
    d_send, d_recv, e_send, e_recv, p_send, p_recv, y_send, y_recv,
    r_send, r_recv, c_send, c_recv, s_send, s_recv, f_send, f_recv,
    a_send, a_recv, b_send, b_recv, h_send, h_recv,
):
    me = lax.axis_index("ep")
    lane = lax.axis_index("tp")
    core = lax.rem(lane, 2)
    side = lane // 2
    other_core, other_side = 1 - core, 1 - side
    partner = 2 * side + other_core
    across = 2 * other_side + core
    capacity, width = send_own.shape[1:]
    half = n_ep // 2
    tokens = xa.shape[0]
    moe_tokens = xe.shape[0]
    kv_local, ext_rows, pair = kd.shape
    q_cols = q_s.shape[1]
    hidden_cols = wd.shape[0]

    def local(i, src, dst):
        return pltpu.make_async_copy(src, dst, l_sem.at[i])

    kw = wk_hbm.shape[1]
    loads = [
        local(0, wg_hbm, wgu.at[:, 0:hidden_cols]),
        local(1, wu_hbm, wgu.at[:, hidden_cols : 2 * hidden_cols]),
        local(2, wd_hbm, wd),
        local(3, xa_hbm, xa),
        local(4, wq_hbm, wqkv.at[:, 0:q_cols]),
        local(5, wk_hbm, wqkv.at[:, q_cols : q_cols + kw]),
        local(6, wv_hbm, wqkv.at[:, q_cols + kw : q_cols + 2 * kw]),
        local(7, wo_hbm, wo),
    ]
    small = [
        pltpu.make_async_copy(src, dst, s_sem.at[i])
        for i, (src, dst) in enumerate(
            [
                (routes_hbm, routes_t),
                (expert_hbm, expert_p),
                (group_hbm, group_p.at[0]),
                (e_gain_hbm, e_gain.at[0]),
                (a_gain_hbm, a_gain.at[0]),
                (q_gain_hbm, q_gain.at[0]),
                (k_gain_hbm, k_gain.at[0]),
                (sink_hbm, sink),
            ]
        )
    ]
    for copy in small:
        copy.start()
    first_rows = moe_tokens // XE_PIECES
    pieces = [
        pltpu.make_async_copy(
            xe_hbm.at[i * first_rows : (i + 1) * first_rows],
            xe.at[i * first_rows : (i + 1) * first_rows],
            x_sem.at[i],
        )
        for i in range(XE_PIECES)
    ]
    for copy in pieces:
        copy.start()

    barrier = pltpu.get_barrier_semaphore()

    def greet(k, carry):
        pl.semaphore_signal(
            barrier, inc=1, device_id={"ep": flip(me, k, n_ep), "tp": lane}, device_id_type=MESH
        )
        return carry

    lax.fori_loop(1, n_ep, greet, 0)
    for peer in (partner, across):
        pl.semaphore_signal(barrier, inc=1, device_id={"ep": me, "tp": peer}, device_id_type=MESH)

    def remote(src, dst, sends, recvs, k, ep, tp):
        return pltpu.make_async_remote_copy(
            src_ref=src,
            dst_ref=dst,
            send_sem=sends.at[k],
            recv_sem=recvs.at[k],
            device_id={"ep": ep, "tp": tp},
            device_id_type=MESH,
        )

    def dispatch(k):
        dest = flip(me, k, n_ep)
        return remote(send_own.at[k], rows_buf.at[lane, k], d_send, d_recv, k, dest, lane)

    def dispatch_other(k):
        dest = flip(me, k, n_ep)
        return remote(send_other.at[k], rows_buf.at[across, k], e_send, e_recv, k, dest, lane)

    def to_partner(k):
        block = rows_buf.at[lane, k]
        return remote(block, block, p_send, p_recv, k, me, partner)

    def to_across(k):
        block = rows_buf.at[lane, k]
        return remote(block, block, y_send, y_recv, k, me, across)

    def relay(k):
        block = rows_buf.at[across, k]
        return remote(block, block, r_send, r_recv, k, me, partner)

    def sum_core(k):
        return remote(part_out.at[k], part_in.at[k], c_send, c_recv, k, me, partner)

    def sum_side(k):
        return remote(y_out.at[k], y_in.at[k], s_send, s_recv, k, me, across)

    def give_back(k):
        return remote(final.at[k], back.at[k], f_send, f_recv, k, flip(me, k, n_ep), lane)

    def attn_core(s):
        return remote(
            attn_ref.at[2 * s + other_core], attn_in.at[s], a_send, a_recv, s, me, partner
        )

    chunk_rows = attn_y_out.shape[1]

    def attn_side(c):
        return remote(attn_y_out.at[c], attn_y_in.at[c], b_send, b_recv, c, me, across)

    def halo_up():
        return remote(
            kv.at[tokens - WINDOW : tokens], halo.at[0], h_send, h_recv, 0, me + 1, lane
        )

    def halo_down():
        return remote(kv.at[0:WINDOW], halo.at[1], h_send, h_recv, 1, me - 1, lane)

    def plan():
        names = iota((n_ep, moe_tokens), 0)
        named = None
        share = jnp.zeros((n_ep, moe_tokens), f32)
        top = routes_t.shape[0]
        prob_sum = expert_p[0:1, :]
        for j in range(1, top):
            prob_sum = prob_sum + expert_p[j : j + 1, :]
        for j in range(top):
            chosen = routes_t[j : j + 1, :] == names
            weight = group_p[...] * expert_p[j : j + 1, :] / prob_sum
            share = share + jnp.where(chosen, weight, 0.0)
            named = chosen if named is None else named | chosen
        before = one_zero(iota((moe_tokens, moe_tokens), 0) < iota((moe_tokens, moe_tokens), 1))
        same = one_zero(iota((moe_tokens, moe_tokens), 0) == iota((moe_tokens, moe_tokens), 1))
        rank = jnp.where(named, dot(one_zero(named), before), -1.0)
        rank_s[...] = rank
        rank_tn[...] = dot_nt(same, rank.astype(bf16))
        share_tn[...] = dot_nt(same, share.astype(bf16))

    def pick(k):
        row = rank_s[pl.ds(flip(me, k, n_ep), 1), :]
        return one_zero(row == iota((capacity, moe_tokens), 0).astype(f32))

    def gathered(chosen, quarter):
        start = pl.multiple_of(quarter * width, width)
        return dot(chosen, xe[:, pl.ds(start, width)]).astype(bf16)

    def D(k, near):
        chosen = pick(k)
        send_own[k] = gathered(chosen, lane)
        dispatch(k).start()
        if near:
            send_other[k] = gathered(chosen, across)
            dispatch_other(k).start()

    def L0():
        chosen = pick(0)
        rows_buf[lane, 0] = gathered(chosen, lane)
        to_partner(0).start()
        rows_buf[across, 0] = gathered(chosen, across)
        relay(0).start()

    def build_mix(part):
        columns = iota((moe_tokens, n_ep), 1)
        slots = iota((moe_tokens, capacity), 1).astype(f32)

        def body(e, carry):
            rank = jnp.sum(jnp.where(columns == e, rank_tn[...], 0.0), axis=1, keepdims=True)
            share = jnp.sum(jnp.where(columns == e, share_tn[...], 0.0), axis=1, keepdims=True)
            mix[e] = jnp.where(rank == slots, share, 0.0).astype(bf16)
            return carry

        lax.fori_loop(part * (n_ep // 2), (part + 1) * (n_ep // 2), body, 0)

    def A(k, near):
        dispatch(k).wait_recv()
        if not near:
            to_across(k).start()
        to_partner(k).start()

    def Z(k):
        dispatch_other(k).wait_recv()
        relay(k).start()

    def B(k):
        to_across(k).wait_recv()
        relay(k).start()

    def C(k):
        to_partner(k).wait_recv()
        relay(k).wait_recv()
        rows = jnp.concatenate([rows_buf[q, k] for q in range(4)], axis=1)
        acts = dot(rows, wgu[...])
        gate, up = acts[:, 0:hidden_cols], acts[:, hidden_cols:]
        hidden = (gate / (1.0 + jnp.exp(-gate)) * up).astype(bf16)
        for c, target in ((other_core, part_out), (core, part_keep)):
            for s in range(2):
                start = pl.multiple_of((2 * s + c) * width, width)
                target[k, s] = dot(hidden, wd[:, pl.ds(start, width)]).astype(bf16)
            if target is part_out:
                sum_core(k).start()

    def E(k):
        sum_core(k).wait_recv()
        y_out[k] = (
            part_keep[k, other_side].astype(f32) + part_in[k, other_side].astype(f32)
        ).astype(bf16)
        sum_side(k).start()
        y_own[k] = part_keep[k, side].astype(f32) + part_in[k, side].astype(f32)

    def F(k, own):
        sum_side(k).wait_recv()
        final[k] = (y_own[k] + y_in[k].astype(f32)).astype(bf16)
        if own:
            total[...] = dot(mix[me], final[0])
        else:
            give_back(k).start()

    def G(k):
        give_back(k).wait_recv()
        total[...] += dot(mix[flip(me, k, n_ep)], back[k])

    def rope_tables():
        lanes = lax.rem(iota((GRID_W, pair), 1), HEAD_DIM // 2)
        quarter = HEAD_DIM // 4
        inverse = jnp.exp(lax.rem(lanes, quarter).astype(f32) * (-LOG_BASE / quarter))
        by_row = lanes < quarter
        grid_rows = tokens // GRID_W
        first = me * grid_rows
        col_angle = iota((GRID_W, pair), 0).astype(f32) * inverse
        row_angle = (iota((grid_rows, pair), 0) + first).astype(f32) * inverse[0:grid_rows]
        for table, fn in ((ctab, jnp.cos), (stab, jnp.sin)):
            cols, rows = fn(col_angle), fn(row_angle)
            for r in range(grid_rows):
                table[r * GRID_W : (r + 1) * GRID_W, :] = jnp.where(
                    by_row, rows[r : r + 1, :], cols
                )

    def qkv(first, last):
        step = tokens // 2
        lanes = iota((1, pair), 1)
        low = lax.rem(lanes, HEAD_DIM) < HEAD_DIM // 2
        ones = one_zero(
            lax.rem(iota((2 * pair, pair), 0), pair) // HEAD_DIM
            == iota((2 * pair, pair), 1) // HEAD_DIM
        )
        gain_q = jnp.concatenate([q_gain[...]] * (pair // HEAD_DIM), axis=1)
        gain_k = jnp.concatenate([k_gain[...]] * (pair // HEAD_DIM), axis=1)

        def turned(x, gain, rows):
            square = x * x
            high = square.astype(bf16)
            rest = (square - high.astype(f32)).astype(bf16)
            mean = dot(jnp.concatenate([high, rest], axis=1), ones) * (1.0 / HEAD_DIM)
            scaled = x * lax.rsqrt(mean + EPSILON) * gain
            swapped = jnp.where(
                low,
                -pltpu.roll(scaled, pair - HEAD_DIM // 2, 1),
                pltpu.roll(scaled, HEAD_DIM // 2, 1),
            )
            return scaled * ctab[rows, :] + swapped * stab[rows, :]

        def body(i, carry):
            rows = pl.ds(pl.multiple_of(i * step, step), step)
            x = dot(xa[rows, :], wqkv[...])
            for g in range(q_cols // pair):
                span = slice(g * pair, (g + 1) * pair)
                q_s[rows, span] = (
                    turned(x[:, span], gain_q, rows) * HEAD_DIM ** (-0.5)
                ).astype(bf16)
            for g in range(kw // pair):
                span = slice(g * pair, (g + 1) * pair)
                k_span = slice(q_cols + g * pair, q_cols + (g + 1) * pair)
                kv[rows, span] = turned(x[:, k_span], gain_k, rows).astype(bf16)
            kv[rows, kw : 2 * kw] = x[:, q_cols + kw :].astype(bf16)
            return carry

        lax.fori_loop(first, last, body, 0)

    def expand(src, start, rows):
        block = jnp.concatenate([src[:, 0:kw], src[:, kw : 2 * kw]], axis=0)
        source = iota((kw, kv_local * pair), 0)
        column = iota((kw, kv_local * pair), 1)
        spread = one_zero(source == column // pair * HEAD_DIM + lax.rem(column, HEAD_DIM))
        doubled = dot(block, spread).astype(bf16)
        for h in range(kv_local):
            span = slice(h * pair, (h + 1) * pair)
            kd[h, start : start + rows, :] = doubled[0:rows, span]
            ve[h, start : start + rows, 0:pair] = doubled[rows:, span]
            ve[h, start : start + rows, pair : 2 * pair] = jnp.ones((rows, pair), bf16)

    def blank(start):
        for h in range(kv_local):
            kd[h, start : start + WINDOW, :] = jnp.zeros((WINDOW, pair), bf16)
            ve[h, start : start + WINDOW, :] = jnp.zeros((WINDOW, 2 * pair), bf16)

    def halo_start():
        @pl.when(me < n_ep - 1)
        def _():
            halo_up().start()

        @pl.when(me > 0)
        def _():
            halo_down().start()

    def halo_finish():
        @pl.when(me > 0)
        def _():
            halo_up().wait_recv()
            expand(halo.at[0], 0, WINDOW)

        @pl.when(me == 0)
        def _():
            blank(0)

        @pl.when(me < n_ep - 1)
        def _():
            halo_down().wait_recv()
            expand(halo.at[1], WINDOW + tokens, WINDOW)

        @pl.when(me == n_ep - 1)
        def _():
            blank(WINDOW + tokens)

    def attend(first, count, stride):
        span = 3 * WINDOW
        lanes = iota((1, pair), 1)
        left = one_zero(lanes < HEAD_DIM)
        right = one_zero(lanes >= HEAD_DIM)
        query = lax.rem(iota((2 * WINDOW, span), 0), WINDOW)
        key = iota((2 * WINDOW, span), 1)
        seen = (key >= query) & (key <= query + 2 * WINDOW)

        def body(j, carry):
            start = pl.multiple_of((first + stride * j) * WINDOW, WINDOW)
            rows = pl.ds(start, WINDOW)
            keys = pl.ds(start, span)
            for h in range(kv_local):
                cols = slice(h * pair, (h + 1) * pair)
                heads = q_s[rows, cols]
                stacked = jnp.concatenate([heads * left, heads * right], axis=0)
                scores = dot_nt(stacked, kd[h, keys, :])
                weights = jnp.where(seen, jnp.exp(scores), 0.0).astype(bf16)
                mixed = dot(weights, ve[h, keys, :])
                sink_0 = jnp.exp(jnp.full((1, pair), sink[2 * h], f32))
                sink_1 = jnp.exp(jnp.full((1, pair), sink[2 * h + 1], f32))
                upper = mixed[0:WINDOW, 0:pair] / (mixed[0:WINDOW, pair:] + sink_0)
                lower = mixed[WINDOW:, 0:pair] / (mixed[WINDOW:, pair:] + sink_1)
                att[rows, cols] = jnp.where(lanes < HEAD_DIM, upper, lower).astype(bf16)
            return carry

        lax.fori_loop(0, count, body, 0)

    def project(part):
        tile = 2 * pair
        quarter = attn_ref.shape[1]

        def body(n, carry):
            cols = pl.ds(pl.multiple_of(n * tile, tile), tile)
            x = dot(att[...], wo[:, cols]).astype(bf16)
            for s in range(attn_ref.shape[0]):
                attn_ref[s, :, cols] = x[s * quarter : (s + 1) * quarter]
            return carry

        count = wo.shape[1] // tile // 2
        lax.fori_loop(part * count, (part + 1) * count, body, 0)
        if part == 1:
            attn_core(0).start()
            attn_core(1).start()

    def attn_sum():
        attn_core(0).wait_recv()
        attn_core(1).wait_recv()

    def attn_cross(c):
        rows = slice(c * chunk_rows, (c + 1) * chunk_rows)
        attn_y_out[c] = (
            attn_ref[2 * other_side + core, rows].astype(f32)
            + attn_in[other_side, rows].astype(f32)
        ).astype(bf16)
        attn_side(c).start()

    def attn_final(c):
        rows = slice(c * chunk_rows, (c + 1) * chunk_rows)
        attn_side(c).wait_recv()
        attn_out_ref[rows] = (
            attn_ref[2 * side + core, rows].astype(f32)
            + attn_in[side, rows].astype(f32)
            + attn_y_in[c].astype(f32)
        ).astype(bf16)

    nb = tokens // WINDOW

    for copy in small[0:4]:
        copy.wait()
    plan()
    for i, copy in enumerate(pieces):
        copy.wait()
        if i == XE_PIECES - 1:
            for load in loads[0:8]:
                load.start()
        rms_inplace(xe, i * first_rows, first_rows, e_gain)
    pl.semaphore_wait(barrier, n_ep + 1)

    def load_ffn():
        for copy in loads[0:3]:
            copy.wait()

    def front_norm():
        for copy in small[4:8]:
            copy.wait()
        loads[3].wait()
        rms_inplace(xa, 0, tokens, a_gain)

    def front_qkv(part):
        if part == 0:
            for copy in loads[4:8]:
                copy.wait()
            rope_tables()
        qkv(part, part + 1)

    if n_ep == 8:
        inner = lax.rem(me // (n_ep // 4) + 1, 4) // 2

        @pl.when(inner == 1)
        def _():
            D(5, False)
            L0()
            D(1, True)
            D(2, True)
            D(6, False)
            load_ffn()
            C(0)
            front_norm()
            front_qkv(0)
            E(0)
            D(3, True)
            A(5, False)
            B(5)
            front_qkv(1)
            D(7, False)
            A(6, False)
            C(5)
            D(4, False)
            expand(kv, WINDOW, tokens)
            E(5)
            halo_start()
            A(4, False)
            B(6)
            A(3, True)
            C(6)
            Z(1)
            A(7, False)
            Z(3)
            attend(1, nb - 2, 1)
            A(2, True)
            A(1, True)
            build_mix(0)
            E(6)
            B(4)
            C(3)
            C(1)
            B(7)
            halo_finish()
            E(3)
            C(4)
            E(1)
            F(6, False)
            attend(0, 2, nb - 1)
            C(7)
            F(5, False)
            E(4)
            project(0)
            F(3, False)
            Z(2)
            build_mix(1)
            project(1)
            C(2)
            E(7)
            attn_sum()
            F(1, False)
            F(4, False)
            attn_cross(6)
            attn_cross(3)
            E(2)
            attn_cross(4)
            attn_cross(7)
            attn_cross(2)
            F(7, False)
            attn_final(6)
            attn_cross(0)
            attn_cross(1)
            attn_final(4)
            attn_final(3)
            F(0, True)
            G(3)
            F(2, False)
            G(2)
            G(7)
            G(1)
            attn_cross(5)
            attn_final(0)
            attn_final(1)
            G(5)
            G(6)
            attn_final(2)
            attn_final(7)
            attn_final(5)
            G(4)

        @pl.when(inner == 0)
        def _():
            D(5, False)
            L0()
            D(1, True)
            front_norm()
            load_ffn()
            C(0)
            D(6, False)
            E(0)
            front_qkv(0)
            D(3, True)
            front_qkv(1)
            A(1, True)
            A(6, False)
            Z(1)
            build_mix(0)
            A(5, False)
            D(4, False)
            C(1)
            E(1)
            B(6)
            build_mix(1)
            D(2, True)
            C(6)
            B(5)
            E(6)
            expand(kv, WINDOW, tokens)
            halo_start()
            Z(2)
            C(5)
            D(7, False)
            A(3, True)
            Z(3)
            E(5)
            attend(1, nb - 2, 1)
            C(3)
            halo_finish()
            A(2, True)
            F(6, False)
            A(4, False)
            attend(0, 2, nb - 1)
            project(0)
            project(1)
            E(3)
            F(5, False)
            B(4)
            A(7, False)
            C(2)
            attn_sum()
            attn_cross(6)
            F(0, True)
            attn_cross(3)
            E(2)
            F(3, False)
            B(7)
            attn_cross(4)
            C(4)
            C(7)
            E(7)
            F(1, False)
            E(4)
            F(2, False)
            attn_cross(5)
            F(7, False)
            attn_cross(2)
            attn_final(4)
            G(5)
            attn_cross(0)
            F(4, False)
            attn_final(3)
            attn_cross(1)
            attn_cross(7)
            attn_final(1)
            attn_final(5)
            attn_final(2)
            G(3)
            attn_final(6)
            attn_final(0)
            G(7)
            G(4)
            G(1)
            G(2)
            G(6)
            attn_final(7)

    else:
        def each(low, high, fn):
            def body(k, carry):
                fn(k)
                return carry

            lax.fori_loop(low, high, body, 0)

        each(half, n_ep, lambda k: D(k, False))
        each(1, half, lambda k: D(k, True))
        L0()
        load_ffn()
        front_norm()
        front_qkv(0)
        front_qkv(1)
        halo_start()
        expand(kv, WINDOW, tokens)
        attend(1, nb - 2, 1)
        each(1, half, lambda k: A(k, True))
        each(1, half, Z)
        each(half, n_ep, lambda k: A(k, False))
        halo_finish()
        attend(0, 2, nb - 1)
        project(0)
        project(1)
        build_mix(0)
        build_mix(1)
        each(half, n_ep, B)
        each(0, n_ep, C)
        each(0, n_ep, E)
        attn_sum()
        F(0, True)
        each(1, n_ep, lambda k: F(k, False))
        for c in range(ATTN_CHUNKS):
            attn_cross(c)
        each(1, n_ep, G)
        for c in range(ATTN_CHUNKS):
            attn_final(c)

    out_ref[...] = total[...].astype(bf16)

    def drain(k, carry):
        @pl.when(k > 0)
        def _():
            dispatch(k).wait_send()
            give_back(k).wait_send()

        to_partner(k).wait_send()

        @pl.when(k >= half)
        def _():
            to_across(k).wait_send()

        @pl.when((k > 0) & (k < half))
        def _():
            dispatch_other(k).wait_send()

        relay(k).wait_send()
        sum_core(k).wait_send()
        sum_side(k).wait_send()
        return carry

    lax.fori_loop(0, n_ep, drain, 0)
    attn_core(0).wait_send()
    attn_core(1).wait_send()
    for c in range(ATTN_CHUNKS):
        attn_side(c).wait_send()

    @pl.when(me < n_ep - 1)
    def _():
        halo_up().wait_send()

    @pl.when(me > 0)
    def _():
        halo_down().wait_send()


def per_device(
    x_attend, attend_gain, w_query, w_key, w_value, query_gain, key_gain, sink_logit, w_output,
    x_experts, expert_gain, routes, group_prob, expert_prob, w_gate, w_up, w_down,
):
    tokens, model_width = x_attend.shape
    q_cols, kv_cols = w_query.shape[1], w_key.shape[1]
    kv_local = kv_cols // HEAD_DIM
    tp_count, n_ep = lax.axis_size("tp"), lax.axis_size("ep")
    moe_rows, top_count = routes.shape
    capacity = max(2, (3 * moe_rows * top_count + 2 * n_ep - 1) // (2 * n_ep))
    col_width = model_width // tp_count
    hidden_cols = w_gate.shape[2]
    slice_rows = tokens // tp_count
    ext = tokens + 2 * WINDOW
    pair = 2 * HEAD_DIM
    chunk = slice_rows // ATTN_CHUNKS
    vmem = pl.BlockSpec(memory_space=pltpu.VMEM)
    hbm = pl.BlockSpec(memory_space=pl.ANY)
    dma = pltpu.SemaphoreType.DMA

    def buf(*shape, dtype=bf16):
        return pltpu.VMEM(shape, dtype)

    expert_out, attend_out = pl.pallas_call(
        functools.partial(fused_kernel, n_ep),
        out_shape=(buf(moe_rows, col_width), buf(slice_rows, model_width)),
        in_specs=[hbm] * 17,
        out_specs=(vmem, vmem),
        scratch_shapes=[
            buf(tokens, model_width),
            buf(model_width, q_cols + 2 * kv_cols),
            buf(q_cols, model_width),
            buf(moe_rows, model_width),
            buf(model_width, 2 * hidden_cols),
            buf(hidden_cols, model_width),
            buf(tokens, pair, dtype=f32),
            buf(tokens, pair, dtype=f32),
            buf(tokens, q_cols),
            buf(tokens, 2 * kv_cols),
            buf(2, WINDOW, 2 * kv_cols),
            buf(kv_local, ext, pair),
            buf(kv_local, ext, 2 * pair),
            buf(tokens, q_cols),
            buf(tp_count, slice_rows, model_width),
            buf(2, slice_rows, model_width),
            buf(ATTN_CHUNKS, chunk, model_width),
            buf(ATTN_CHUNKS, chunk, model_width),
            buf(1, model_width, dtype=f32),
            buf(1, HEAD_DIM, dtype=f32),
            buf(1, HEAD_DIM, dtype=f32),
            pltpu.SMEM(sink_logit.shape, f32),
            buf(1, model_width, dtype=f32),
            buf(top_count, moe_rows, dtype=i32),
            buf(top_count, moe_rows, dtype=f32),
            buf(1, moe_rows, dtype=f32),
            buf(n_ep, moe_rows, dtype=f32),
            buf(moe_rows, n_ep, dtype=f32),
            buf(moe_rows, n_ep, dtype=f32),
            buf(n_ep, moe_rows, capacity),
            buf(n_ep, capacity, col_width),
            buf(n_ep // 2, capacity, col_width),
            buf(tp_count, n_ep, capacity, col_width),
            buf(n_ep, 2, capacity, col_width),
            buf(n_ep, 2, capacity, col_width),
            buf(n_ep, 2, capacity, col_width),
            buf(n_ep, capacity, col_width),
            buf(n_ep, capacity, col_width, dtype=f32),
            buf(n_ep, capacity, col_width),
            buf(n_ep, capacity, col_width),
            buf(n_ep, capacity, col_width),
            buf(moe_rows, col_width, dtype=f32),
            dma((8,)),
            dma((XE_PIECES,)),
            dma((8,)),
        ]
        + [dma((n_ep,))] * 16
        + [dma((2,))] * 2
        + [dma((ATTN_CHUNKS,))] * 2
        + [dma((2,))] * 2,
        compiler_params=pltpu.CompilerParams(
            collective_id=0, has_side_effects=True, vmem_limit_bytes=60 * 1024 * 1024
        ),
    )(
        x_attend, attend_gain, w_query, w_key, w_value, query_gain, key_gain,
        sink_logit, w_output, x_experts, expert_gain, routes.T, group_prob,
        expert_prob.T, w_gate[0], w_up[0], w_down[0],
    )
    return (attend_out, expert_out)


def solution(mesh):
    placed = (
        P("ep", None),
        P(),
        P(None, "tp"),
        P(None, "tp"),
        P(None, "tp"),
        P(),
        P(),
        P("tp"),
        P("tp", None),
        P("ep", None),
        P(),
        P("ep", None),
        P("ep"),
        P("ep", None),
        P("ep", None, "tp"),
        P("ep", None, "tp"),
        P("ep", "tp", None),
    )
    return jax.shard_map(
        per_device,
        mesh=mesh,
        in_specs=placed,
        out_specs=(P(("ep", "tp"), None), P("ep", "tp")),
        check_vma=False,
    )
```

```python
import functools

import jax
import jax.numpy as jnp
from jax import lax
from jax.experimental import pallas as pl
from jax.experimental.pallas import tpu as pltpu
from jax.sharding import PartitionSpec as P

HEAD_DIM = 64
WINDOW = 128
GRID_W = 64
MESH = pl.DeviceIdType.MESH
EPSILON = 1e-06
LOG_BASE = 9.210340371976184
ATTN_CHUNKS = 8
XE_PIECES = 3
bf16, f32, i32 = jnp.bfloat16, jnp.float32, jnp.int32


def flip(a, b, count):
    total, bit = 0, 1
    while bit < count:
        total = total + lax.rem(a // bit + b // bit, 2) * bit
        bit *= 2
    return total


def iota(shape, dim):
    return lax.broadcasted_iota(i32, shape, dim)


def dot(a, b):
    return jnp.dot(a, b, preferred_element_type=f32)


def dot_nt(a, b):
    return lax.dot_general(a, b, (((1,), (1,)), ((), ())), preferred_element_type=f32)


def one_zero(mask):
    return jnp.where(mask, 1.0, 0.0).astype(bf16)


def rms_inplace(ref, first, count, gain_ref):
    chunk, lanes = 64, 128
    features = ref.shape[1]
    steps = 2 if count % (2 * chunk) == 0 else 1

    def body(i, carry):
        for j in range(steps):
            start = first + (i * steps + j) * chunk
            rows = pl.ds(pl.multiple_of(start, chunk), chunk)
            v = ref[rows, :].astype(f32)
            square = v * v
            part = square[:, 0:lanes]
            for c in range(lanes, features, lanes):
                part = part + square[:, c : c + lanes]
            mean = jnp.sum(part, axis=-1, keepdims=True) * (1.0 / features)
            ref[rows, :] = (v * lax.rsqrt(mean + EPSILON) * gain_ref[...]).astype(bf16)
        return carry

    lax.fori_loop(0, count // (chunk * steps), body, 0)


def fused_kernel(
    n_ep,
    xa_hbm, a_gain_hbm, wq_hbm, wk_hbm, wv_hbm, q_gain_hbm, k_gain_hbm, sink_hbm, wo_hbm,
    xe_hbm, e_gain_hbm, routes_hbm, group_hbm, expert_hbm, wg_hbm, wu_hbm, wd_hbm,
    out_ref, attn_out_ref,
    xa, wqkv, wo, xe, wgu, wd,
    ctab, stab, q_s, kv, halo, kd, ve, att,
    attn_ref, attn_in, attn_y_out, attn_y_in,
    a_gain, q_gain, k_gain, sink, e_gain, routes_t, expert_p,
    group_p, rank_s, rank_tn, share_tn, mix,
    send_own, send_other, rows_buf, part_out, part_keep, part_in,
    y_out, y_own, y_in, final, back, total,
    l_sem, x_sem, s_sem,
    d_send, d_recv, e_send, e_recv, p_send, p_recv, y_send, y_recv,
    r_send, r_recv, c_send, c_recv, s_send, s_recv, f_send, f_recv,
    a_send, a_recv, b_send, b_recv, h_send, h_recv,
):
    me = lax.axis_index("ep")
    lane = lax.axis_index("tp")
    core = lax.rem(lane, 2)
    side = lane // 2
    other_core, other_side = 1 - core, 1 - side
    partner = 2 * side + other_core
    across = 2 * other_side + core
    capacity, width = send_own.shape[1:]
    half = n_ep // 2
    tokens = xa.shape[0]
    moe_tokens = xe.shape[0]
    kv_local, ext_rows, pair = kd.shape
    q_cols = q_s.shape[1]
    hidden_cols = wd.shape[0]

    def local(i, src, dst):
        return pltpu.make_async_copy(src, dst, l_sem.at[i])

    kw = wk_hbm.shape[1]
    loads = [
        local(0, wg_hbm, wgu.at[:, 0:hidden_cols]),
        local(1, wu_hbm, wgu.at[:, hidden_cols : 2 * hidden_cols]),
        local(2, wd_hbm, wd),
        local(3, xa_hbm, xa),
        local(4, wq_hbm, wqkv.at[:, 0:q_cols]),
        local(5, wk_hbm, wqkv.at[:, q_cols : q_cols + kw]),
        local(6, wv_hbm, wqkv.at[:, q_cols + kw : q_cols + 2 * kw]),
        local(7, wo_hbm, wo),
    ]
    small = [
        pltpu.make_async_copy(src, dst, s_sem.at[i])
        for i, (src, dst) in enumerate(
            [
                (routes_hbm, routes_t),
                (expert_hbm, expert_p),
                (group_hbm, group_p.at[0]),
                (e_gain_hbm, e_gain.at[0]),
                (a_gain_hbm, a_gain.at[0]),
                (q_gain_hbm, q_gain.at[0]),
                (k_gain_hbm, k_gain.at[0]),
                (sink_hbm, sink),
            ]
        )
    ]
    barrier = pltpu.get_barrier_semaphore()

    def greet(k, carry):
        pl.semaphore_signal(
            barrier, inc=1, device_id={"ep": flip(me, k, n_ep), "tp": lane}, device_id_type=MESH
        )
        return carry

    lax.fori_loop(1, n_ep, greet, 0)
    for peer in (partner, across):
        pl.semaphore_signal(barrier, inc=1, device_id={"ep": me, "tp": peer}, device_id_type=MESH)

    for copy in small:
        copy.start()
    first_rows = moe_tokens // XE_PIECES
    pieces = [
        pltpu.make_async_copy(
            xe_hbm.at[i * first_rows : (i + 1) * first_rows],
            xe.at[i * first_rows : (i + 1) * first_rows],
            x_sem.at[i],
        )
        for i in range(XE_PIECES)
    ]
    for copy in pieces:
        copy.start()

    def remote(src, dst, sends, recvs, k, ep, tp):
        return pltpu.make_async_remote_copy(
            src_ref=src,
            dst_ref=dst,
            send_sem=sends.at[k],
            recv_sem=recvs.at[k],
            device_id={"ep": ep, "tp": tp},
            device_id_type=MESH,
        )

    def dispatch(k):
        dest = flip(me, k, n_ep)
        return remote(send_own.at[k], rows_buf.at[lane, k], d_send, d_recv, k, dest, lane)

    def dispatch_other(k):
        dest = flip(me, k, n_ep)
        return remote(send_other.at[k], rows_buf.at[across, k], e_send, e_recv, k, dest, lane)

    def to_partner(k):
        block = rows_buf.at[lane, k]
        return remote(block, block, p_send, p_recv, k, me, partner)

    def to_across(k):
        block = rows_buf.at[lane, k]
        return remote(block, block, y_send, y_recv, k, me, across)

    def relay(k):
        block = rows_buf.at[across, k]
        return remote(block, block, r_send, r_recv, k, me, partner)

    def sum_core(k):
        return remote(part_out.at[k], part_in.at[k], c_send, c_recv, k, me, partner)

    def sum_side(k):
        return remote(y_out.at[k], y_in.at[k], s_send, s_recv, k, me, across)

    def give_back(k):
        return remote(final.at[k], back.at[k], f_send, f_recv, k, flip(me, k, n_ep), lane)

    def attn_core(s):
        return remote(
            attn_ref.at[2 * s + other_core], attn_in.at[s], a_send, a_recv, s, me, partner
        )

    chunk_rows = attn_y_out.shape[1]

    def attn_side(c):
        return remote(attn_y_out.at[c], attn_y_in.at[c], b_send, b_recv, c, me, across)

    def halo_up():
        return remote(
            kv.at[tokens - WINDOW : tokens], halo.at[0], h_send, h_recv, 0, me + 1, lane
        )

    def halo_down():
        return remote(kv.at[0:WINDOW], halo.at[1], h_send, h_recv, 1, me - 1, lane)

    def plan():
        names = iota((n_ep, moe_tokens), 0)
        named = None
        share = jnp.zeros((n_ep, moe_tokens), f32)
        top = routes_t.shape[0]
        prob_sum = expert_p[0:1, :]
        for j in range(1, top):
            prob_sum = prob_sum + expert_p[j : j + 1, :]
        for j in range(top):
            chosen = routes_t[j : j + 1, :] == names
            weight = group_p[...] * expert_p[j : j + 1, :] / prob_sum
            share = share + jnp.where(chosen, weight, 0.0)
            named = chosen if named is None else named | chosen
        before = one_zero(iota((moe_tokens, moe_tokens), 0) < iota((moe_tokens, moe_tokens), 1))
        same = one_zero(iota((moe_tokens, moe_tokens), 0) == iota((moe_tokens, moe_tokens), 1))
        rank = jnp.where(named, dot(one_zero(named), before), -1.0)
        rank_s[...] = rank
        rank_tn[...] = dot_nt(same, rank.astype(bf16))
        share_tn[...] = dot_nt(same, share.astype(bf16))

    def pick(k):
        row = rank_s[pl.ds(flip(me, k, n_ep), 1), :]
        return one_zero(row == iota((capacity, moe_tokens), 0).astype(f32))

    def gathered(chosen, quarter):
        start = pl.multiple_of(quarter * width, width)
        return dot(chosen, xe[:, pl.ds(start, width)]).astype(bf16)

    def D(k, near):
        chosen = pick(k)
        send_own[k] = gathered(chosen, lane)
        dispatch(k).start()
        if near:
            send_other[k] = gathered(chosen, across)
            dispatch_other(k).start()

    def L0():
        chosen = pick(0)
        rows_buf[lane, 0] = gathered(chosen, lane)
        to_partner(0).start()
        rows_buf[across, 0] = gathered(chosen, across)
        relay(0).start()

    def build_mix(part):
        columns = iota((moe_tokens, n_ep), 1)
        slots = iota((moe_tokens, capacity), 1).astype(f32)

        def body(e, carry):
            rank = jnp.sum(jnp.where(columns == e, rank_tn[...], 0.0), axis=1, keepdims=True)
            share = jnp.sum(jnp.where(columns == e, share_tn[...], 0.0), axis=1, keepdims=True)
            mix[e] = jnp.where(rank == slots, share, 0.0).astype(bf16)
            return carry

        lax.fori_loop(part * (n_ep // 2), (part + 1) * (n_ep // 2), body, 0)

    def A(k, near):
        dispatch(k).wait_recv()
        if not near:
            to_across(k).start()
        to_partner(k).start()

    def Z(k):
        dispatch_other(k).wait_recv()
        relay(k).start()

    def B(k):
        to_across(k).wait_recv()
        relay(k).start()

    def C(k):
        to_partner(k).wait_recv()
        relay(k).wait_recv()
        rows = jnp.concatenate([rows_buf[q, k] for q in range(4)], axis=1)
        acts = dot(rows, wgu[...])
        gate, up = acts[:, 0:hidden_cols], acts[:, hidden_cols:]
        hidden = (gate / (1.0 + jnp.exp(-gate)) * up).astype(bf16)
        for c, target in ((other_core, part_out), (core, part_keep)):
            for s in range(2):
                start = pl.multiple_of((2 * s + c) * width, width)
                target[k, s] = dot(hidden, wd[:, pl.ds(start, width)]).astype(bf16)
            if target is part_out:
                sum_core(k).start()

    def E(k):
        sum_core(k).wait_recv()
        y_out[k] = (
            part_keep[k, other_side].astype(f32) + part_in[k, other_side].astype(f32)
        ).astype(bf16)
        sum_side(k).start()
        y_own[k] = part_keep[k, side].astype(f32) + part_in[k, side].astype(f32)

    def F(k, own):
        sum_side(k).wait_recv()
        final[k] = (y_own[k] + y_in[k].astype(f32)).astype(bf16)
        if own:
            total[...] = dot(mix[me], final[0])
        else:
            give_back(k).start()

    def G(k):
        give_back(k).wait_recv()
        total[...] += dot(mix[flip(me, k, n_ep)], back[k])

    def rope_tables():
        lanes = lax.rem(iota((GRID_W, pair), 1), HEAD_DIM // 2)
        quarter = HEAD_DIM // 4
        inverse = jnp.exp(lax.rem(lanes, quarter).astype(f32) * (-LOG_BASE / quarter))
        by_row = lanes < quarter
        grid_rows = tokens // GRID_W
        first = me * grid_rows
        col_angle = iota((GRID_W, pair), 0).astype(f32) * inverse
        row_angle = (iota((grid_rows, pair), 0) + first).astype(f32) * inverse[0:grid_rows]
        for table, fn in ((ctab, jnp.cos), (stab, jnp.sin)):
            cols, rows = fn(col_angle), fn(row_angle)
            for r in range(grid_rows):
                table[r * GRID_W : (r + 1) * GRID_W, :] = jnp.where(
                    by_row, rows[r : r + 1, :], cols
                )

    def qkv(first, last):
        step = tokens // 2
        lanes = iota((1, pair), 1)
        low = lax.rem(lanes, HEAD_DIM) < HEAD_DIM // 2
        ones = one_zero(
            lax.rem(iota((2 * pair, pair), 0), pair) // HEAD_DIM
            == iota((2 * pair, pair), 1) // HEAD_DIM
        )
        gain_q = jnp.concatenate([q_gain[...]] * (pair // HEAD_DIM), axis=1)
        gain_k = jnp.concatenate([k_gain[...]] * (pair // HEAD_DIM), axis=1)

        def turned(x, gain, rows):
            square = x * x
            high = square.astype(bf16)
            rest = (square - high.astype(f32)).astype(bf16)
            mean = dot(jnp.concatenate([high, rest], axis=1), ones) * (1.0 / HEAD_DIM)
            scaled = x * lax.rsqrt(mean + EPSILON) * gain
            swapped = jnp.where(
                low,
                -pltpu.roll(scaled, pair - HEAD_DIM // 2, 1),
                pltpu.roll(scaled, HEAD_DIM // 2, 1),
            )
            return scaled * ctab[rows, :] + swapped * stab[rows, :]

        def body(i, carry):
            rows = pl.ds(pl.multiple_of(i * step, step), step)
            x = dot(xa[rows, :], wqkv[...])
            for g in range(q_cols // pair):
                span = slice(g * pair, (g + 1) * pair)
                q_s[rows, span] = (
                    turned(x[:, span], gain_q, rows) * HEAD_DIM ** (-0.5)
                ).astype(bf16)
            for g in range(kw // pair):
                span = slice(g * pair, (g + 1) * pair)
                k_span = slice(q_cols + g * pair, q_cols + (g + 1) * pair)
                kv[rows, span] = turned(x[:, k_span], gain_k, rows).astype(bf16)
            kv[rows, kw : 2 * kw] = x[:, q_cols + kw :].astype(bf16)
            return carry

        lax.fori_loop(first, last, body, 0)

    def expand(src, start, rows):
        block = jnp.concatenate([src[:, 0:kw], src[:, kw : 2 * kw]], axis=0)
        source = iota((kw, kv_local * pair), 0)
        column = iota((kw, kv_local * pair), 1)
        spread = one_zero(source == column // pair * HEAD_DIM + lax.rem(column, HEAD_DIM))
        doubled = dot(block, spread).astype(bf16)
        for h in range(kv_local):
            span = slice(h * pair, (h + 1) * pair)
            kd[h, start : start + rows, :] = doubled[0:rows, span]
            ve[h, start : start + rows, 0:pair] = doubled[rows:, span]
            ve[h, start : start + rows, pair : 2 * pair] = jnp.ones((rows, pair), bf16)

    def blank(start):
        for h in range(kv_local):
            kd[h, start : start + WINDOW, :] = jnp.zeros((WINDOW, pair), bf16)
            ve[h, start : start + WINDOW, :] = jnp.zeros((WINDOW, 2 * pair), bf16)

    def halo_start():
        @pl.when(me < n_ep - 1)
        def _():
            halo_up().start()

        @pl.when(me > 0)
        def _():
            halo_down().start()

    def halo_finish():
        @pl.when(me > 0)
        def _():
            halo_up().wait_recv()
            expand(halo.at[0], 0, WINDOW)

        @pl.when(me == 0)
        def _():
            blank(0)

        @pl.when(me < n_ep - 1)
        def _():
            halo_down().wait_recv()
            expand(halo.at[1], WINDOW + tokens, WINDOW)

        @pl.when(me == n_ep - 1)
        def _():
            blank(WINDOW + tokens)

    def attend(first, count, stride):
        span = 3 * WINDOW
        lanes = iota((1, pair), 1)
        left = one_zero(lanes < HEAD_DIM)
        right = one_zero(lanes >= HEAD_DIM)
        query = lax.rem(iota((2 * WINDOW, span), 0), WINDOW)
        key = iota((2 * WINDOW, span), 1)
        seen = (key >= query) & (key <= query + 2 * WINDOW)

        def body(j, carry):
            start = pl.multiple_of((first + stride * j) * WINDOW, WINDOW)
            rows = pl.ds(start, WINDOW)
            keys = pl.ds(start, span)
            for h in range(kv_local):
                cols = slice(h * pair, (h + 1) * pair)
                heads = q_s[rows, cols]
                stacked = jnp.concatenate([heads * left, heads * right], axis=0)
                scores = dot_nt(stacked, kd[h, keys, :])
                weights = jnp.where(seen, jnp.exp(scores), 0.0).astype(bf16)
                mixed = dot(weights, ve[h, keys, :])
                sink_0 = jnp.exp(jnp.full((1, pair), sink[2 * h], f32))
                sink_1 = jnp.exp(jnp.full((1, pair), sink[2 * h + 1], f32))
                upper = mixed[0:WINDOW, 0:pair] / (mixed[0:WINDOW, pair:] + sink_0)
                lower = mixed[WINDOW:, 0:pair] / (mixed[WINDOW:, pair:] + sink_1)
                att[rows, cols] = jnp.where(lanes < HEAD_DIM, upper, lower).astype(bf16)
            return carry

        lax.fori_loop(0, count, body, 0)

    def project(part):
        tile = 2 * pair
        quarter = attn_ref.shape[1]

        def body(n, carry):
            cols = pl.ds(pl.multiple_of(n * tile, tile), tile)
            x = dot(att[...], wo[:, cols]).astype(bf16)
            for s in range(attn_ref.shape[0]):
                attn_ref[s, :, cols] = x[s * quarter : (s + 1) * quarter]
            return carry

        count = wo.shape[1] // tile // 2
        lax.fori_loop(part * count, (part + 1) * count, body, 0)
        if part == 1:
            attn_core(0).start()
            attn_core(1).start()

    def attn_sum():
        attn_core(0).wait_recv()
        attn_core(1).wait_recv()

    def attn_cross(c):
        rows = slice(c * chunk_rows, (c + 1) * chunk_rows)
        attn_y_out[c] = (
            attn_ref[2 * other_side + core, rows].astype(f32)
            + attn_in[other_side, rows].astype(f32)
        ).astype(bf16)
        attn_side(c).start()

    def attn_final(c):
        rows = slice(c * chunk_rows, (c + 1) * chunk_rows)
        attn_side(c).wait_recv()
        attn_out_ref[rows] = (
            attn_ref[2 * side + core, rows].astype(f32)
            + attn_in[side, rows].astype(f32)
            + attn_y_in[c].astype(f32)
        ).astype(bf16)

    nb = tokens // WINDOW

    for copy in small[0:4]:
        copy.wait()
    plan()
    for i, copy in enumerate(pieces):
        copy.wait()
        if i == XE_PIECES - 1:
            for load in loads[0:8]:
                load.start()
        rms_inplace(xe, i * first_rows, first_rows, e_gain)
    pl.semaphore_wait(barrier, n_ep + 1)

    def load_ffn():
        for copy in loads[0:3]:
            copy.wait()

    def front_norm():
        for copy in small[4:8]:
            copy.wait()
        loads[3].wait()
        rms_inplace(xa, 0, tokens, a_gain)

    def front_qkv(part):
        if part == 0:
            for copy in loads[4:8]:
                copy.wait()
            rope_tables()
        qkv(part, part + 1)

    if n_ep == 8:
        inner = lax.rem(me // (n_ep // 4) + 1, 4) // 2

        @pl.when(inner == 1)
        def _():
            D(5, False)
            L0()
            D(1, True)
            D(2, True)
            D(6, False)
            load_ffn()
            C(0)
            front_norm()
            front_qkv(0)
            E(0)
            D(3, True)
            A(5, False)
            B(5)
            front_qkv(1)
            D(7, False)
            A(6, False)
            C(5)
            D(4, False)
            expand(kv, WINDOW, tokens)
            E(5)
            halo_start()
            A(4, False)
            B(6)
            A(3, True)
            C(6)
            Z(1)
            A(7, False)
            Z(3)
            attend(1, nb - 2, 1)
            A(2, True)
            A(1, True)
            build_mix(0)
            E(6)
            B(4)
            C(3)
            C(1)
            B(7)
            halo_finish()
            E(3)
            C(4)
            E(1)
            F(6, False)
            attend(0, 2, nb - 1)
            C(7)
            F(5, False)
            E(4)
            project(0)
            F(3, False)
            Z(2)
            build_mix(1)
            project(1)
            C(2)
            E(7)
            attn_sum()
            F(1, False)
            F(4, False)
            attn_cross(6)
            attn_cross(3)
            E(2)
            attn_cross(4)
            attn_cross(7)
            attn_cross(2)
            F(7, False)
            attn_final(6)
            attn_cross(0)
            attn_cross(1)
            attn_final(4)
            attn_final(3)
            F(0, True)
            G(3)
            F(2, False)
            G(2)
            G(7)
            G(1)
            attn_cross(5)
            attn_final(0)
            attn_final(1)
            G(5)
            G(6)
            attn_final(2)
            attn_final(7)
            attn_final(5)
            G(4)

        @pl.when(inner == 0)
        def _():
            D(5, False)
            L0()
            D(1, True)
            front_norm()
            load_ffn()
            C(0)
            D(6, False)
            E(0)
            front_qkv(0)
            D(3, True)
            front_qkv(1)
            A(1, True)
            A(6, False)
            Z(1)
            build_mix(0)
            A(5, False)
            D(4, False)
            C(1)
            E(1)
            B(6)
            build_mix(1)
            D(2, True)
            C(6)
            B(5)
            E(6)
            expand(kv, WINDOW, tokens)
            halo_start()
            Z(2)
            C(5)
            D(7, False)
            A(3, True)
            Z(3)
            E(5)
            attend(1, nb - 2, 1)
            C(3)
            halo_finish()
            A(2, True)
            F(6, False)
            A(4, False)
            attend(0, 2, nb - 1)
            project(0)
            project(1)
            E(3)
            F(5, False)
            B(4)
            A(7, False)
            C(2)
            attn_sum()
            attn_cross(6)
            F(0, True)
            attn_cross(3)
            E(2)
            F(3, False)
            B(7)
            attn_cross(4)
            C(4)
            C(7)
            E(7)
            F(1, False)
            E(4)
            F(2, False)
            attn_cross(5)
            F(7, False)
            attn_cross(2)
            attn_final(4)
            G(5)
            attn_cross(0)
            F(4, False)
            attn_final(3)
            attn_cross(1)
            attn_cross(7)
            attn_final(1)
            attn_final(5)
            attn_final(2)
            G(3)
            attn_final(6)
            attn_final(0)
            G(7)
            G(4)
            G(1)
            G(2)
            G(6)
            attn_final(7)

    else:
        def each(low, high, fn):
            def body(k, carry):
                fn(k)
                return carry

            lax.fori_loop(low, high, body, 0)

        each(half, n_ep, lambda k: D(k, False))
        each(1, half, lambda k: D(k, True))
        L0()
        load_ffn()
        front_norm()
        front_qkv(0)
        front_qkv(1)
        halo_start()
        expand(kv, WINDOW, tokens)
        attend(1, nb - 2, 1)
        each(1, half, lambda k: A(k, True))
        each(1, half, Z)
        each(half, n_ep, lambda k: A(k, False))
        halo_finish()
        attend(0, 2, nb - 1)
        project(0)
        project(1)
        build_mix(0)
        build_mix(1)
        each(half, n_ep, B)
        each(0, n_ep, C)
        each(0, n_ep, E)
        attn_sum()
        F(0, True)
        each(1, n_ep, lambda k: F(k, False))
        for c in range(ATTN_CHUNKS):
            attn_cross(c)
        each(1, n_ep, G)
        for c in range(ATTN_CHUNKS):
            attn_final(c)

    out_ref[...] = total[...].astype(bf16)

    def drain(k, carry):
        @pl.when(k > 0)
        def _():
            dispatch(k).wait_send()
            give_back(k).wait_send()

        to_partner(k).wait_send()

        @pl.when(k >= half)
        def _():
            to_across(k).wait_send()

        @pl.when((k > 0) & (k < half))
        def _():
            dispatch_other(k).wait_send()

        relay(k).wait_send()
        sum_core(k).wait_send()
        sum_side(k).wait_send()
        return carry

    lax.fori_loop(0, n_ep, drain, 0)
    attn_core(0).wait_send()
    attn_core(1).wait_send()
    for c in range(ATTN_CHUNKS):
        attn_side(c).wait_send()

    @pl.when(me < n_ep - 1)
    def _():
        halo_up().wait_send()

    @pl.when(me > 0)
    def _():
        halo_down().wait_send()


def per_device(
    x_attend, attend_gain, w_query, w_key, w_value, query_gain, key_gain, sink_logit, w_output,
    x_experts, expert_gain, routes, group_prob, expert_prob, w_gate, w_up, w_down,
):
    tokens, model_width = x_attend.shape
    q_cols, kv_cols = w_query.shape[1], w_key.shape[1]
    kv_local = kv_cols // HEAD_DIM
    tp_count, n_ep = lax.axis_size("tp"), lax.axis_size("ep")
    moe_rows, top_count = routes.shape
    capacity = max(2, (3 * moe_rows * top_count + 2 * n_ep - 1) // (2 * n_ep))
    col_width = model_width // tp_count
    hidden_cols = w_gate.shape[2]
    slice_rows = tokens // tp_count
    ext = tokens + 2 * WINDOW
    pair = 2 * HEAD_DIM
    chunk = slice_rows // ATTN_CHUNKS
    vmem = pl.BlockSpec(memory_space=pltpu.VMEM)
    hbm = pl.BlockSpec(memory_space=pl.ANY)
    dma = pltpu.SemaphoreType.DMA

    def buf(*shape, dtype=bf16):
        return pltpu.VMEM(shape, dtype)

    expert_out, attend_out = pl.pallas_call(
        functools.partial(fused_kernel, n_ep),
        out_shape=(buf(moe_rows, col_width), buf(slice_rows, model_width)),
        in_specs=[hbm] * 17,
        out_specs=(vmem, vmem),
        scratch_shapes=[
            buf(tokens, model_width),
            buf(model_width, q_cols + 2 * kv_cols),
            buf(q_cols, model_width),
            buf(moe_rows, model_width),
            buf(model_width, 2 * hidden_cols),
            buf(hidden_cols, model_width),
            buf(tokens, pair, dtype=f32),
            buf(tokens, pair, dtype=f32),
            buf(tokens, q_cols),
            buf(tokens, 2 * kv_cols),
            buf(2, WINDOW, 2 * kv_cols),
            buf(kv_local, ext, pair),
            buf(kv_local, ext, 2 * pair),
            buf(tokens, q_cols),
            buf(tp_count, slice_rows, model_width),
            buf(2, slice_rows, model_width),
            buf(ATTN_CHUNKS, chunk, model_width),
            buf(ATTN_CHUNKS, chunk, model_width),
            buf(1, model_width, dtype=f32),
            buf(1, HEAD_DIM, dtype=f32),
            buf(1, HEAD_DIM, dtype=f32),
            pltpu.SMEM(sink_logit.shape, f32),
            buf(1, model_width, dtype=f32),
            buf(top_count, moe_rows, dtype=i32),
            buf(top_count, moe_rows, dtype=f32),
            buf(1, moe_rows, dtype=f32),
            buf(n_ep, moe_rows, dtype=f32),
            buf(moe_rows, n_ep, dtype=f32),
            buf(moe_rows, n_ep, dtype=f32),
            buf(n_ep, moe_rows, capacity),
            buf(n_ep, capacity, col_width),
            buf(n_ep // 2, capacity, col_width),
            buf(tp_count, n_ep, capacity, col_width),
            buf(n_ep, 2, capacity, col_width),
            buf(n_ep, 2, capacity, col_width),
            buf(n_ep, 2, capacity, col_width),
            buf(n_ep, capacity, col_width),
            buf(n_ep, capacity, col_width, dtype=f32),
            buf(n_ep, capacity, col_width),
            buf(n_ep, capacity, col_width),
            buf(n_ep, capacity, col_width),
            buf(moe_rows, col_width, dtype=f32),
            dma((8,)),
            dma((XE_PIECES,)),
            dma((8,)),
        ]
        + [dma((n_ep,))] * 16
        + [dma((2,))] * 2
        + [dma((ATTN_CHUNKS,))] * 2
        + [dma((2,))] * 2,
        compiler_params=pltpu.CompilerParams(
            collective_id=0, has_side_effects=True, vmem_limit_bytes=60 * 1024 * 1024
        ),
    )(
        x_attend, attend_gain, w_query, w_key, w_value, query_gain, key_gain,
        sink_logit, w_output, x_experts, expert_gain, routes.T, group_prob,
        expert_prob.T, w_gate[0], w_up[0], w_down[0],
    )
    return (attend_out, expert_out)


def solution(mesh):
    placed = (
        P("ep", None),
        P(),
        P(None, "tp"),
        P(None, "tp"),
        P(None, "tp"),
        P(),
        P(),
        P("tp"),
        P("tp", None),
        P("ep", None),
        P(),
        P("ep", None),
        P("ep"),
        P("ep", None),
        P("ep", None, "tp"),
        P("ep", None, "tp"),
        P("ep", "tp", None),
    )
    return jax.shard_map(
        per_device,
        mesh=mesh,
        in_specs=placed,
        out_specs=(P(("ep", "tp"), None), P("ep", "tp")),
        check_vma=False,
    )
```
